32 devices in a mesh: ep: 8 (over z, y), tp: 4 (over x, core).
Axes of the slice: x: 2, y: 2, z: 4, core: 2. Of those that a mesh axis runs over, the one named last changes fastest.
Arguments:
- glu_value: bfloat16 [4096, 1024], P('ep', 'tp'), may hold values from -6 to 6
- glu_gate: bfloat16 [4096, 1024], P('ep', 'tp'), may hold values from -12 to 12
- conv_kernel: float32 [31, 1024], P(None, 'tp'), may hold values from -11.49474 to 11.49474
- ln_gain: float32 [1024], P('tp'), may hold values from 0.1 to 1.9
- out_weight: bfloat16 [1024, 2048], P('tp'), may hold values from -0.1875 to 0.1875
- moe_input: bfloat16 [2048, 2048], P('ep'), may hold values from -6 to 6
- moe_gain: float32 [2048], replicated, may hold values from 0.1 to 1.9
- gate_weight: bfloat16 [8, 2048, 3072], P('ep', None, 'tp'), may hold values from -0.125 to 0.125
- up_weight: bfloat16 [8, 2048, 3072], P('ep', None, 'tp'), may hold values from -0.125 to 0.125
- down_weight: bfloat16 [8, 3072, 2048], P('ep', 'tp'), may hold values from -0.109375 to 0.109375
- expert_ids: int32 [2048, 2], P('ep'), may hold values from 0 to 7, all different within a row; in each aligned block of 256 rows (0 to 255, 256 to 511, ...) at most 128 rows name the same one
- route_weight: float32 [2048, 2], P('ep'), may hold values from 0.2 to 1
Outputs:
- mixer_out: bfloat16 [4096, 2048], P(('ep', 'tp'))
- expert_out: bfloat16 [2048, 2048], P('ep', 'tp')
The draws below stay inside these ranges and needn't reach their ends.
Inputs may be any that keep to these rules, and one draw needn't show every extreme that they name: `expert_ids`: each row names 2 different experts. In the rows of one device no expert is named by more than 128 rows; the bound is reached at some expert in some device's rows.
All inputs are finite; a program needn't handle non-finite values.
Results may differ from the reference program's by a relative error of at most 0.012.
Values may be sent and summed in bfloat16 or wider, within the bound.
A program may use at most 64 MiB of HBM per device.

```python
import math
import jax
import jax.numpy as jnp
import numpy as np
from jax import lax

D = 2048
MIX = 1024
KERNEL = 31
FF = 3072
TOP = 2
TOKB_DEV = 256
EXPERTS = 8
CAP = 128
TOKA = 4096
TOKB = 2048
N_EP = 8
N_TP = 4


def draw_conv_kernel(key, part):
    base_key = jax.random.fold_in(key, 17)
    rough_key = jax.random.fold_in(key, 29)
    position = jnp.arange(MIX, dtype=jnp.float32) / MIX
    rough = jnp.exp(jax.random.uniform(rough_key, (MIX,), jnp.float32, math.log(0.6), math.log(1.6)))
    scale = jnp.exp(position * math.log(10.0)) * rough * KERNEL ** (-0.5)
    base = jnp.clip(jax.random.normal(base_key, (KERNEL, MIX), jnp.float32), -4.0, 4.0)
    return (base * scale[None, :]).astype(jnp.float32)


def level_of(key, shape, shards, low, high):
    def one(axis_at, shards_of):
        heights = jax.random.uniform(jax.random.fold_in(jax.random.fold_in(key, 6), axis_at), (shards_of,), jnp.float32, low / len(shards), high / len(shards))
        return jnp.repeat(jnp.exp(heights), shape[axis_at] // shards_of).reshape((-1,) + (1,) * (len(shape) - axis_at - 1))

    level = one(*shards[0])
    for cut in shards[1:]:
        level = level * one(*cut)
    return level


def shared_out(key, own, number, rows, number_of, top, reach, skew):
    ranking = jax.random.permutation(key, number_of)
    crowded, ordinary = load_shares(number_of, rows * top, reach, skew, True), load_shares(number_of, rows * top, reach, skew, False)
    places = jnp.arange(number_of)

    def named(tallies, offset_by):
        used = int((tallies > 0).sum())
        fixed = max(1, used // 4)
        moved = fixed + (places - fixed + offset_by * (used - fixed)) % max(1, number_of - fixed)
        return jnp.zeros((number_of,), jnp.int32).at[ranking[jnp.where(places < fixed, places, moved)]].set(jnp.asarray(tallies, jnp.int32))

    tallies = jnp.where(number % 4 == 0, named(crowded, number // 4), named(ordinary, number - number // 4 - 1))
    mixed = jax.random.permutation(jax.random.fold_in(own, 3), number_of)
    donor, receiver = mixed[0:number_of // 2 * 2:2], mixed[1:number_of // 2 * 2:2]
    margin = jnp.minimum(tallies[donor] - 1, reach - tallies[receiver]) // 2
    margin = jnp.where((donor == ranking[0]) | (receiver == ranking[0]) | (tallies[receiver] == 0), 0, jnp.maximum(margin, 0))
    moved = jax.random.randint(jax.random.fold_in(own, 4), (number_of // 2,), 0, 1 << 20) % (margin + 1)
    tallies = tallies.at[donor].add(-moved).at[receiver].add(moved)
    members = jnp.searchsorted(jnp.cumsum(tallies), jnp.arange(rows * top), side="right").astype(jnp.int32)
    grid = members.reshape(top, rows).T
    grid = grid[jax.random.permutation(jax.random.fold_in(own, 1), rows)]
    offset_by = jax.random.randint(jax.random.fold_in(own, 2), (rows, 1), 0, top)
    return jnp.take_along_axis(grid, (jnp.arange(top)[None, :] + offset_by) % top, axis=1)


def load_shares(number_of, total, most, skew, full):
    portions = [(1 << 20) // math.isqrt(rank ** skew) + 1 for rank in range(1, number_of + 1)]
    largest = most if full else min(most, max(-(-total // number_of), total * portions[0] // sum(portions)))
    least = 1 if total - largest >= number_of - 1 else 0
    counts, rest = [largest] + [least] * (number_of - 1), total - largest - least * (number_of - 1)
    while rest > 0:
        movable = [i for i in range(1, number_of) if counts[i] < largest] or [i for i in range(1, number_of) if counts[i] < most]
        pool, budget = sum([portions[i] for i in movable]), rest
        for i in movable:
            extra = min(most - counts[i], max(1, budget * portions[i] // pool), rest)
            counts[i] = counts[i] + extra
            rest = rest - extra
    return np.array(counts)


def normal_values(key, shape, scale, limit, pieces=(), kind=jnp.bfloat16):
    entries = scale * jax.random.normal(key, shape, jnp.float32)
    if pieces:
        entries = entries * level_of(key, shape, pieces, -0.22, 0.18)
    return jnp.clip(entries, -limit, limit).astype(kind)


def setup_inputs(seed: int = 0) -> dict:
    streams_of = jax.random.split(jax.random.key(seed), 13)
    glu_value = normal_values(streams_of[0], (TOKA, MIX), 1.0, 6.0, ((0, 8), (1, 4)))
    glu_gate = normal_values(streams_of[1], (TOKA, MIX), 2.0, 12.0, ((0, 8), (1, 4)))
    conv_kernel = draw_conv_kernel(jax.random.fold_in(streams_of[12], 71), 0)
    ln_gain = jnp.clip(1.0 + 0.18 * jax.random.normal(streams_of[3], (MIX,), jnp.float32), 0.1, 1.9)
    out_weight = normal_values(streams_of[4], (MIX, D), MIX ** -0.5, 0.1875, ((0, 4),))
    moe_input = normal_values(streams_of[5], (TOKB, D), 1.0, 6.0, ((0, 8),))
    moe_gain = jnp.clip(1.0 + 0.18 * jax.random.normal(streams_of[6], (D,), jnp.float32), 0.1, 1.9)
    gate_weight = normal_values(streams_of[7], (EXPERTS, D, FF), D ** -0.5, 0.125, ((0, 8), (2, 4)))
    up_weight = normal_values(streams_of[8], (EXPERTS, D, FF), D ** -0.5, 0.125, ((0, 8), (2, 4)))
    down_weight = normal_values(streams_of[9], (EXPERTS, FF, D), FF ** -0.5, 0.109375, ((0, 8), (1, 4)))
    expert_ids_keys = jax.random.split(jax.random.fold_in(streams_of[10], 1), TOKB // TOKB_DEV)
    expert_ids_turns = jax.random.permutation(jax.random.fold_in(streams_of[10], 3), TOKB // TOKB_DEV)
    expert_ids = jax.vmap(lambda own, number: shared_out(jax.random.fold_in(streams_of[10], 2), own, number, TOKB_DEV, EXPERTS, TOP, CAP, 1))(expert_ids_keys, expert_ids_turns).reshape((TOKB, TOP))
    route_weight = jnp.clip(0.2 + 0.8 * jax.random.uniform(streams_of[11], (TOKB, TOP), jnp.float32) ** level_of(streams_of[11], (TOKB, TOP), ((0, 8),), -0.2, 0.2), 0.2, 1.0)
    return {"glu_value": glu_value, "glu_gate": glu_gate, "conv_kernel": conv_kernel, "ln_gain": ln_gain, "out_weight": out_weight, "moe_input": moe_input, "moe_gain": moe_gain, "gate_weight": gate_weight, "up_weight": up_weight, "down_weight": down_weight, "expert_ids": expert_ids, "route_weight": route_weight}


eps_rms = 1e-06
eps_norm = 1e-05

def slot_numbers(expert_ids, experts, capacity):
    chosen = expert_ids.reshape(-1)
    onehot = (chosen[:, None] == jnp.arange(experts, dtype=jnp.int32)[None, :]).astype(jnp.int32)
    earlier = jnp.cumsum(onehot, axis=0) - onehot
    position = lax.optimization_barrier(jnp.sum(earlier * onehot, axis=1))
    return (chosen * capacity + position).astype(jnp.int32)

def fill_slots(normed, slot_index, experts, capacity, chosen_per_token):
    owners = jnp.full((experts * capacity,), -1, jnp.int32)
    token_of = (jnp.arange(slot_index.shape[0], dtype=jnp.int32) // chosen_per_token).astype(jnp.int32)
    owners = owners.at[slot_index].set(token_of)
    picked = jnp.take(normed, jnp.maximum(owners, 0), axis=0)
    filled = jnp.where((owners >= 0)[:, None], picked, jnp.zeros_like(picked))
    return filled.reshape(experts, capacity, normed.shape[1])

def mixer_half(glu_value, glu_gate, conv_kernel, ln_gain, out_weight):
    gated = (glu_value.astype(jnp.float32) * jax.nn.sigmoid(glu_gate.astype(jnp.float32))).astype(jnp.bfloat16)
    length = gated.shape[0]
    padded = jnp.concatenate([jnp.zeros((KERNEL - 1, MIX), jnp.bfloat16), gated], axis=0).astype(jnp.float32)
    convolved = jnp.zeros((length, MIX), jnp.float32)
    for tap_index in range(KERNEL):
        begin = KERNEL - 1 - tap_index
        convolved = convolved + conv_kernel[tap_index] * padded[begin:begin + length]
    total = lax.optimization_barrier(jnp.sum(convolved, axis=1))
    squares = lax.optimization_barrier(jnp.sum(convolved * convolved, axis=1))
    mean = total / MIX
    variance = squares / MIX - mean * mean
    scaled = (convolved - mean[:, None]) * lax.rsqrt(variance + eps_norm)[:, None] * ln_gain
    activated = jax.nn.silu(scaled).astype(jnp.bfloat16)
    group = MIX // N_TP
    result = jnp.zeros((length, D), jnp.float32)
    for part_index in range(N_TP):
        partial_sum = jnp.dot(activated[:, part_index * group:(part_index + 1) * group], out_weight[part_index * group:(part_index + 1) * group], preferred_element_type=jnp.float32).astype(jnp.bfloat16)
        result = result + partial_sum.astype(jnp.float32)
    return result.astype(jnp.bfloat16)

def run_expert(operands):
    arrived, w_gate, w_up, w_down = operands
    gate_act = jnp.dot(arrived, w_gate, preferred_element_type=jnp.float32)
    up_act = jnp.dot(arrived, w_up, preferred_element_type=jnp.float32)
    hidden = (jax.nn.silu(gate_act) * up_act).astype(jnp.bfloat16)
    group = FF // N_TP
    total = jnp.zeros((arrived.shape[0], D), jnp.float32)
    for part_index in range(N_TP):
        partial_sum = jnp.dot(hidden[:, part_index * group:(part_index + 1) * group], w_down[part_index * group:(part_index + 1) * group], preferred_element_type=jnp.float32).astype(jnp.bfloat16)
        total = total + partial_sum.astype(jnp.float32)
    return total.astype(jnp.bfloat16)

def expert_half(moe_input, moe_gain, gate_weight, up_weight, down_weight, expert_ids, route_weight):
    values = moe_input.astype(jnp.float32)
    normed = (values * lax.rsqrt(lax.optimization_barrier(jnp.mean(values * values, axis=1, keepdims=True)) + eps_rms) * moe_gain).astype(jnp.bfloat16)
    normed_blocks = normed.reshape(N_EP, TOKB_DEV, D)
    id_blocks = expert_ids.reshape(N_EP, TOKB_DEV, TOP)
    slot_index = jax.vmap(lambda ids: slot_numbers(ids, EXPERTS, CAP))(id_blocks)
    sent = jax.vmap(lambda block, slots: fill_slots(block, slots, EXPERTS, CAP, TOP))(normed_blocks, slot_index)
    by_expert = jnp.swapaxes(sent, 0, 1).reshape(EXPERTS, N_EP * CAP, D)
    answers = lax.map(run_expert, (by_expert, gate_weight, up_weight, down_weight))
    answers = jnp.swapaxes(answers.reshape(EXPERTS, N_EP, CAP, D), 0, 1).reshape(N_EP, EXPERTS * CAP, D)

    def combine(block_answers, slots, weights):
        picked = jnp.take(block_answers, slots, axis=0).astype(jnp.float32).reshape(TOKB_DEV, TOP, D)
        return lax.optimization_barrier(jnp.sum(picked * weights[:, :, None], axis=1))
    mixed = jax.vmap(combine)(answers, slot_index, route_weight.reshape(N_EP, TOKB_DEV, TOP))
    return mixed.reshape(N_EP * TOKB_DEV, D).astype(jnp.bfloat16)

def reference(glu_value, glu_gate, conv_kernel, ln_gain, out_weight, moe_input, moe_gain, gate_weight, up_weight, down_weight, expert_ids, route_weight):
    mixer_out = mixer_half(glu_value, glu_gate, conv_kernel, ln_gain, out_weight)
    expert_out = expert_half(moe_input, moe_gain, gate_weight, up_weight, down_weight, expert_ids, route_weight)
    return (mixer_out, expert_out)
```

```python
import functools

import jax
import jax.numpy as jnp
from jax import lax
from jax.experimental import pallas as pl
from jax.experimental.pallas import tpu as pltpu
from jax.sharding import PartitionSpec as P

eps_rms = 1e-06
eps_norm = 1e-05
MESH = pl.DeviceIdType.MESH
f32 = jnp.float32
bf16 = jnp.bfloat16


def kernel(
    n,
    tp,
    cap,
    group,
    reach,
    moe_hbm,
    moe_gain_hbm,
    ids_t_hbm,
    route_t_hbm,
    taps_hbm,
    ln_gain_hbm,
    value_hbm,
    gate_hbm,
    w_out_hbm,
    w_gate_hbm,
    w_up_hbm,
    w_down_hbm,
    mixer_ref,
    expert_ref,
    value,
    gate,
    w_out,
    w_gate,
    w_up,
    w_down,
    load_sem,
    normed,
    slots,
    near_slots,
    onehots,
    arrived,
    near_send,
    near_recv,
    fn_send,
    fn_recv,
    a2a_send,
    a2a_recv,
    fx_send,
    fx_recv,
    fp_send,
    fp_recv,
    fq_send,
    fq_recv,
    gated,
    halo_in,
    halo_send,
    halo_recv,
    padded,
    conv,
    stat_out,
    stat_in,
    stat_send,
    stat_recv,
    act,
    mix_out,
    mix_own,
    mix_in,
    mix_send,
    mix_recv,
    mix_x_out,
    mix_x_in,
    mix_x_send,
    mix_x_recv,
    rs_out,
    rs_own,
    rs_in,
    rs_send,
    rs_recv,
    rx_out,
    rx_in,
    rx_send,
    rx_recv,
    answer,
    returned,
    ret_send,
    ret_recv,
    total,
    meta_ref,
    moe_ref,
    moe_gain_ref,
    ids_t_ref,
    route_t_ref,
    taps_ref,
    ln_gain_ref,
    small_sem,
):
    me = lax.axis_index("ep")
    mine = lax.axis_index("tp")
    core = lax.rem(mine, 2)
    chip = mine // 2
    partner = chip * 2 + 1 - core
    chips = tp // 2
    groups = n // group
    rows = group * cap
    tokens, width = moe_ref.shape
    quarter = width // tp
    length, chan = value.shape
    halo = halo_in.shape[0]
    own_rows = length // tp

    def toward(k):
        return lax.rem(me // 2 + k // 2, n // 2) * 2 + lax.rem(me + k, 2)

    def source(k):
        return lax.rem(me // 2 + n // 2 - k // 2, n // 2) * 2 + lax.rem(me + k, 2)

    def block(k):
        return pl.ds(pl.multiple_of(k * cap, cap), cap)

    def columns_of(part):
        return pl.ds(pl.multiple_of(part * quarter, 128), quarter)

    def across(j):
        there = lax.rem(chip + j, chips)
        here = lax.rem(chip + chips - j, chips)
        return there * 2 + core, here * 2 + core

    barrier = pltpu.get_barrier_semaphore()

    def greet_ep(k, _):
        pl.semaphore_signal(
            barrier, inc=1, device_id={"ep": lax.rem(me + k, n)}, device_id_type=MESH
        )
        return 0

    lax.fori_loop(1, n, greet_ep, 0)
    for j in range(1, tp):
        pl.semaphore_signal(
            barrier, inc=1, device_id={"tp": lax.rem(mine + j, tp)}, device_id_type=MESH
        )

    loads = [
        pltpu.make_async_copy(src, dst, load_sem.at[i])
        for i, (src, dst) in enumerate(
            [
                (value_hbm, value),
                (gate_hbm, gate),
                (w_out_hbm, w_out),
                (w_gate_hbm.at[0], w_gate),
                (w_up_hbm.at[0], w_up),
                (w_down_hbm.at[0], w_down),
            ]
        )
    ]
    smalls = [
        pltpu.make_async_copy(src, dst, small_sem.at[i])
        for i, (src, dst) in enumerate(
            [
                (moe_hbm, moe_ref),
                (moe_gain_hbm, moe_gain_ref),
                (ids_t_hbm, ids_t_ref),
                (route_t_hbm, route_t_ref),
                (taps_hbm, taps_ref),
                (ln_gain_hbm, ln_gain_ref),
            ]
        )
    ]
    for load in smalls:
        load.start()
    for load in loads:
        load.start()
    for load in smalls:
        load.wait()
    everything = moe_ref[...].astype(f32)
    inverse = lax.rsqrt(jnp.sum(everything * everything, axis=1, keepdims=True) / width + eps_rms)
    normed[...] = (everything * inverse * moe_gain_ref[...]).astype(bf16)
    lead = lax.broadcasted_iota(jnp.int32, (128, tokens), 0)
    meta = jnp.where(lead == 0, ids_t_ref[0:1, :].astype(f32), 0.0)
    meta = jnp.where(lead == 1, ids_t_ref[1:2, :].astype(f32), meta)
    meta = jnp.where(lead == 2, route_t_ref[0:1, :], meta)
    meta = jnp.where(lead == 3, route_t_ref[1:2, :], meta)
    meta_ref[...] = jnp.transpose(meta)
    row = lax.broadcasted_iota(jnp.int32, (tokens, tokens), 0)
    col = lax.broadcasted_iota(jnp.int32, (tokens, tokens), 1)
    below = (col < row).astype(f32).astype(bf16)
    above = (row < col).astype(f32).astype(bf16)

    def a2a_copy(k):
        return pltpu.make_async_remote_copy(
            src_ref=slots.at[block(k)],
            dst_ref=arrived.at[mine, block(k)],
            send_sem=a2a_send.at[k],
            recv_sem=a2a_recv.at[k],
            device_id={"ep": toward(k)},
            device_id_type=MESH,
        )

    def near_copy(xx):
        return pltpu.make_async_remote_copy(
            src_ref=near_slots.at[xx],
            dst_ref=arrived.at[xx * 2 + core, pl.ds(cap, cap)],
            send_sem=near_send.at[xx],
            recv_sem=near_recv.at[xx],
            device_id={"ep": toward(1)},
            device_id_type=MESH,
        )

    def slot_picks(k):
        expert = toward(k)
        member = jnp.maximum(
            (ids_t_ref[0:1, :] == expert).astype(f32), (ids_t_ref[1:2, :] == expert).astype(f32)
        )
        member = jnp.broadcast_to(member, (cap, tokens))
        place = jnp.dot(member.astype(bf16), above, preferred_element_type=f32)
        slot = lax.broadcasted_iota(jnp.int32, (cap, tokens), 0).astype(f32)
        return jnp.where(place == slot, member, 0.0).astype(bf16)

    def picked(pick, part):
        return jnp.dot(
            pick, normed[:, columns_of(part)], preferred_element_type=f32
        ).astype(bf16)

    pl.semaphore_wait(barrier, n - 1 + tp - 1)

    def dispatch(k, _):
        slots[block(k), :] = picked(slot_picks(k), mine)
        a2a_copy(k).start()
        return 0

    loads[0].wait()
    loads[1].wait()
    gated_now = (value[...].astype(f32) * jax.nn.sigmoid(gate[...].astype(f32))).astype(bf16)
    gated[...] = gated_now
    halo_copy = pltpu.make_async_remote_copy(
        src_ref=gated.at[pl.ds(length - halo, halo)],
        dst_ref=halo_in,
        send_sem=halo_send,
        recv_sem=halo_recv,
        device_id={"ep": lax.rem(me + 1, n)},
        device_id_type=MESH,
    )
    halo_copy.start()
    padded[pl.ds(halo, length), :] = gated_now.astype(f32)

    lax.fori_loop(2, n, dispatch, 0)
    pick = slot_picks(1)
    for xx in range(chips):
        near_slots[xx] = picked(pick, xx * 2 + core)
        near_copy(xx).start()

    pick = slot_picks(0)
    for part in range(tp):
        arrived[part, 0:cap, :] = picked(pick, part)

    def fx_copy(k, j):
        to, _ = across(j)
        return pltpu.make_async_remote_copy(
            src_ref=arrived.at[mine, block(k)],
            dst_ref=arrived.at[mine, block(k)],
            send_sem=fx_send.at[k, j - 1],
            recv_sem=fx_recv.at[k, j - 1],
            device_id={"tp": to},
            device_id_type=MESH,
        )

    def fp_copy(k):
        return pltpu.make_async_remote_copy(
            src_ref=arrived.at[mine, block(k)],
            dst_ref=arrived.at[mine, block(k)],
            send_sem=fp_send.at[k],
            recv_sem=fp_recv.at[k],
            device_id={"tp": partner},
            device_id_type=MESH,
        )

    def fq_copy(k, j):
        _, origin = across(j)
        return pltpu.make_async_remote_copy(
            src_ref=arrived.at[origin, block(k)],
            dst_ref=arrived.at[origin, block(k)],
            send_sem=fq_send.at[k, j - 1],
            recv_sem=fq_recv.at[k, j - 1],
            device_id={"tp": partner},
            device_id_type=MESH,
        )

    def fn_copy(xx):
        return pltpu.make_async_remote_copy(
            src_ref=arrived.at[xx * 2 + core, pl.ds(cap, cap)],
            dst_ref=arrived.at[xx * 2 + core, pl.ds(cap, cap)],
            send_sem=fn_send.at[xx],
            recv_sem=fn_recv.at[xx],
            device_id={"tp": partner},
            device_id_type=MESH,
        )

    def over_group(g, do, first=2):
        def one(k, _):
            @pl.when(k >= first)
            def _():
                do(k)

            return 0

        lax.fori_loop(g * group, (g + 1) * group, one, 0)

    def forward_first(g):
        def one(k):
            a2a_copy(k).wait_recv()
            for j in range(1, chips):
                fx_copy(k, j).start()
            fp_copy(k).start()

        over_group(g, one)

    def forward_second(g):
        def one(k):
            for j in range(1, chips):
                fx_copy(k, j).wait_recv()
                fq_copy(k, j).start()

        over_group(g, one)

    def forward_near():
        for xx in range(chips):
            near_copy(xx).wait_recv()
            fn_copy(xx).start()

    halo_copy.wait_recv()
    padded[pl.ds(0, halo), :] = jnp.where(me == 0, 0.0, halo_in[...].astype(f32))
    step_rows = 64
    window = step_rows + halo

    for lane in range(0, chan, 128):

        def conv_step(i, _):
            base = pl.multiple_of(i * step_rows, step_rows)
            rows_in = padded[pl.ds(base, window), lane : lane + 128]
            result = jnp.zeros((step_rows, 128), f32)
            for shift in range(8):
                turned = rows_in if shift == 0 else pltpu.roll(rows_in, window - shift, 0)
                for tap in range(reach):
                    offset = halo - tap
                    if offset % 8 == shift:
                        begin = offset - shift
                        result = (
                            result
                            + taps_ref[tap : tap + 1, lane : lane + 128]
                            * turned[begin : begin + step_rows]
                        )
            conv[pl.ds(base, step_rows), lane : lane + 128] = result
            return 0

        lax.fori_loop(0, length // step_rows, conv_step, 0)

    convolved = conv[...]
    sums = jnp.sum(convolved, axis=1, keepdims=True)
    squares = jnp.sum(convolved * convolved, axis=1, keepdims=True)
    lanes = lax.broadcasted_iota(jnp.int32, (length, 128), 1)
    packed = jnp.where(lanes == 0, sums, jnp.where(lanes == 1, squares, 0.0))
    stat_out[...] = jnp.transpose(packed)[0:8]

    def stat_copy(j):
        return pltpu.make_async_remote_copy(
            src_ref=stat_out,
            dst_ref=stat_in.at[j - 1],
            send_sem=stat_send.at[j - 1],
            recv_sem=stat_recv.at[j - 1],
            device_id={"tp": lax.rem(mine + j, tp)},
            device_id_type=MESH,
        )

    for j in range(1, tp):
        stat_copy(j).start()

    forward_near()
    forward_first(0)
    if groups > 1:
        forward_first(1)
    forward_second(0)

    stats = stat_out[...]
    for j in range(1, tp):
        stat_copy(j).wait_recv()
        stats = stats + stat_in[j - 1]
    stats = jnp.concatenate([stats, jnp.zeros((120, length), f32)], axis=0)
    columns = jnp.transpose(stats)
    mean = columns[:, 0:1] / (chan * tp)
    variance = columns[:, 1:2] / (chan * tp) - mean * mean
    scaled = (conv[...] - mean) * lax.rsqrt(variance + eps_norm) * ln_gain_ref[...]
    act[...] = jax.nn.silu(scaled).astype(bf16)

    def mix_copy(xx):
        return pltpu.make_async_remote_copy(
            src_ref=mix_out.at[xx],
            dst_ref=mix_in.at[xx],
            send_sem=mix_send.at[xx],
            recv_sem=mix_recv.at[xx],
            device_id={"tp": partner},
            device_id_type=MESH,
        )

    def mix_part(owner):
        begin = pl.multiple_of(owner * own_rows, own_rows)
        return jnp.dot(act[pl.ds(begin, own_rows), :], w_out[...], preferred_element_type=f32)

    loads[2].wait()

    def mix_first(xx, _):
        mix_out[xx] = mix_part(xx * 2 + 1 - core).astype(bf16)
        mix_copy(xx).start()
        return 0

    def mix_second(xx, _):
        mix_own[xx] = mix_part(xx * 2 + core).astype(bf16)
        return 0

    lax.fori_loop(0, chips, mix_first, 0)
    lax.fori_loop(0, chips, mix_second, 0)

    half = own_rows // 2

    def mix_x_copy(j, part):
        to, _ = across(j)
        span = pl.ds(part * half, half)
        return pltpu.make_async_remote_copy(
            src_ref=mix_x_out.at[j - 1, span],
            dst_ref=mix_x_in.at[j - 1, span],
            send_sem=mix_x_send.at[j - 1, part],
            recv_sem=mix_x_recv.at[j - 1, part],
            device_id={"tp": to},
            device_id_type=MESH,
        )

    def mix_stage():
        for xx in range(chips):
            mix_copy(xx).wait_recv()
        for j in range(1, chips):
            there = lax.rem(chip + j, chips)
            mix_x_out[j - 1] = (mix_own[there].astype(f32) + mix_in[there].astype(f32)).astype(
                bf16
            )
    loads[3].wait()
    loads[4].wait()
    loads[5].wait()

    def rs_copy(g, xx):
        return pltpu.make_async_remote_copy(
            src_ref=rs_out.at[g, xx],
            dst_ref=rs_in.at[g, xx],
            send_sem=rs_send.at[g, xx],
            recv_sem=rs_recv.at[g, xx],
            device_id={"tp": partner},
            device_id_type=MESH,
        )

    def rx_copy(k, j):
        to, _ = across(j)
        return pltpu.make_async_remote_copy(
            src_ref=rx_out.at[j - 1, block(k)],
            dst_ref=rx_in.at[j - 1, block(k)],
            send_sem=rx_send.at[k, j - 1],
            recv_sem=rx_recv.at[k, j - 1],
            device_id={"tp": to},
            device_id_type=MESH,
        )

    def ret_copy(k):
        return pltpu.make_async_remote_copy(
            src_ref=answer.at[block(k)],
            dst_ref=returned.at[block(k)],
            send_sem=ret_send.at[k],
            recv_sem=ret_recv.at[k],
            device_id={"ep": source(k)},
            device_id_type=MESH,
        )

    def expert_step(g):
        @pl.when(g == 0)
        def _():
            for xx in range(chips):
                fn_copy(xx).wait_recv()

        def one(k):
            fp_copy(k).wait_recv()
            for j in range(1, chips):
                fq_copy(k, j).wait_recv()

        over_group(g, one)
        span = pl.ds(pl.multiple_of(g * rows, rows), rows)
        x = jnp.concatenate([arrived[part, span] for part in range(tp)], axis=1)
        gate_act = jnp.dot(x, w_gate[...], preferred_element_type=f32)
        up_act = jnp.dot(x, w_up[...], preferred_element_type=f32)
        hidden = (jax.nn.silu(gate_act) * up_act).astype(bf16)
        for xx in range(chips):
            begin = pl.multiple_of((xx * 2 + 1 - core) * quarter, 128)
            rs_out[g, xx] = jnp.dot(
                hidden, w_down[:, pl.ds(begin, quarter)], preferred_element_type=f32
            ).astype(bf16)
            rs_copy(g, xx).start()
        for xx in range(chips):
            begin = pl.multiple_of((xx * 2 + core) * quarter, 128)
            rs_own[g, xx] = jnp.dot(
                hidden, w_down[:, pl.ds(begin, quarter)], preferred_element_type=f32
            ).astype(bf16)

    def sum_step(g):
        for xx in range(chips):
            rs_copy(g, xx).wait_recv()
        span = pl.ds(pl.multiple_of(g * rows, rows), rows)
        for j in range(1, chips):
            there = lax.rem(chip + j, chips)
            rx_out[j - 1, span] = (
                rs_own[g, there].astype(f32) + rs_in[g, there].astype(f32)
            ).astype(bf16)

        def one(k):
            for j in range(1, chips):
                rx_copy(k, j).start()

        over_group(g, one, 0)

    def return_step(g):
        def one(k):
            inner = pl.ds(pl.multiple_of((k - g * group) * cap, cap), cap)
            result = rs_own[g, chip, inner].astype(f32) + rs_in[g, chip, inner].astype(f32)
            for j in range(1, chips):
                rx_copy(k, j).wait_recv()
                result = result + rx_in[j - 1, block(k)].astype(f32)
            answer[block(k), :] = result.astype(bf16)

            @pl.when(k > 0)
            def _():
                ret_copy(k).start()

        over_group(g, one, 0)

    total[...] = jnp.zeros_like(total)

    def combine_step(g):
        def take(k, _):
            @pl.when(k > 0)
            def _():
                ret_copy(k).wait_recv()

            expert = toward(k)
            weight = jnp.where(meta_ref[:, 0:1] == expert.astype(f32), meta_ref[:, 2:3], 0.0) + jnp.where(
                meta_ref[:, 1:2] == expert.astype(f32), meta_ref[:, 3:4], 0.0
            )
            answers = returned[block(k), :]
            total[...] += weight * jnp.dot(onehots[k], answers, preferred_element_type=f32)
            return 0

        lax.fori_loop(g * group, (g + 1) * group, take, 0)

    def place_of(k, _):
        expert = toward(k)
        member = jnp.maximum(
            (meta_ref[:, 0:1] == expert.astype(f32)).astype(f32), (meta_ref[:, 1:2] == expert.astype(f32)).astype(f32)
        )
        member = jnp.broadcast_to(member, (tokens, cap))
        place = jnp.dot(below, member.astype(bf16), preferred_element_type=f32)
        slot = lax.broadcasted_iota(jnp.int32, (tokens, cap), 1).astype(f32)
        onehots[k] = jnp.where(place == slot, member, 0.0).astype(bf16)
        return 0

    def step(g, _):
        @pl.when(g < groups)
        def _():
            expert_step(g)

        @pl.when(g < groups)
        def _():
            sum_step(g)

        @pl.when(g + 1 < groups)
        def _():
            forward_second(g + 1)

        @pl.when(g == groups)
        def _():
            lax.fori_loop(0, n, place_of, 0)

        @pl.when((g >= 1) & (g < groups + 1))
        def _():
            return_step(g - 1)

        @pl.when(g == 0)
        def _():
            mix_stage()

        @pl.when(g + 2 < groups)
        def _():
            forward_first(g + 2)

        @pl.when(g == groups - 1)
        def _():
            for j in range(1, chips):
                mix_x_copy(j, 0).start()
                mix_x_copy(j, 1).start()

        return 0

    lax.fori_loop(0, groups + 1, step, 0)
    returned[0:cap, :] = answer[0:cap, :]

    def combine(g, _):
        combine_step(g)
        return 0

    lax.fori_loop(0, groups, combine, 0)
    expert_ref[...] = total[...].astype(bf16)

    mixed = mix_own[chip].astype(f32) + mix_in[chip].astype(f32)
    for j in range(1, chips):
        mix_x_copy(j, 0).wait_recv()
        mix_x_copy(j, 1).wait_recv()
        mixed = mixed + mix_x_in[j - 1].astype(f32)
    mixer_ref[...] = mixed.astype(bf16)

    ret_copy(1).wait_send()

    def left(k, _):
        a2a_copy(k).wait_send()
        ret_copy(k).wait_send()
        fp_copy(k).wait_send()
        for j in range(1, chips):
            fx_copy(k, j).wait_send()
            fq_copy(k, j).wait_send()
        return 0

    lax.fori_loop(2, n, left, 0)

    def left_x(k, _):
        for j in range(1, chips):
            rx_copy(k, j).wait_send()
        return 0

    lax.fori_loop(0, n, left_x, 0)
    halo_copy.wait_send()
    for j in range(1, tp):
        stat_copy(j).wait_send()
    for xx in range(chips):
        mix_copy(xx).wait_send()
        near_copy(xx).wait_send()
        fn_copy(xx).wait_send()
    for j in range(1, chips):
        mix_x_copy(j, 0).wait_send()
        mix_x_copy(j, 1).wait_send()

    def left_group(g, _):
        for xx in range(chips):
            rs_copy(g, xx).wait_send()
        return 0

    lax.fori_loop(0, groups, left_group, 0)


def on_device(
    glu_value,
    glu_gate,
    conv_kernel,
    ln_gain,
    out_weight,
    moe_input,
    moe_gain,
    gate_weight,
    up_weight,
    down_weight,
    expert_ids,
    route_weight,
):
    n = lax.axis_size("ep")
    tp = lax.axis_size("tp")
    chips = tp // 2
    length, chan = glu_value.shape
    reach = conv_kernel.shape[0]
    halo = -(-(reach - 1) // 16) * 16
    tokens, width = moe_input.shape
    hidden = gate_weight.shape[2]
    cap = 4 * max(1, tokens // n)
    group = max(1, min(n, 256 // cap))
    groups = n // group
    rows = group * cap
    quarter = width // tp
    own_rows = length // tp
    vmem = pl.BlockSpec(memory_space=pltpu.VMEM)
    hbm = pl.BlockSpec(memory_space=pltpu.HBM)
    dma = pltpu.SemaphoreType.DMA
    V = pltpu.VMEM
    others = max(1, chips - 1)
    mixed, routed = pl.pallas_call(
        functools.partial(kernel, n, tp, cap, group, reach),
        out_shape=(
            pltpu.VMEM((own_rows, out_weight.shape[1]), bf16),
            pltpu.VMEM((tokens, quarter), bf16),
        ),
        in_specs=[hbm] * 12,
        out_specs=(vmem, vmem),
        scratch_shapes=[
            V((length, chan), bf16),
            V((length, chan), bf16),
            V(out_weight.shape, bf16),
            V((width, hidden), bf16),
            V((width, hidden), bf16),
            V((hidden, width), bf16),
            dma((6,)),
            V((tokens, width), bf16),
            V((n * cap, quarter), bf16),
            V((chips, cap, quarter), bf16),
            V((n, tokens, cap), bf16),
            V((tp, n * cap, quarter), bf16),
            dma((chips,)),
            dma((chips,)),
            dma((chips,)),
            dma((chips,)),
            dma((n,)),
            dma((n,)),
            dma((n, others)),
            dma((n, others)),
            dma((n,)),
            dma((n,)),
            dma((n, others)),
            dma((n, others)),
            V((length, chan), bf16),
            V((halo, chan), bf16),
            dma,
            dma,
            V((length + halo, chan), f32),
            V((length, chan), f32),
            V((8, length), f32),
            V((tp - 1, 8, length), f32),
            dma((tp - 1,)),
            dma((tp - 1,)),
            V((length, chan), bf16),
            V((chips, own_rows, out_weight.shape[1]), bf16),
            V((chips, own_rows, out_weight.shape[1]), bf16),
            V((chips, own_rows, out_weight.shape[1]), bf16),
            dma((chips,)),
            dma((chips,)),
            V((others, own_rows, out_weight.shape[1]), bf16),
            V((others, own_rows, out_weight.shape[1]), bf16),
            dma((others, 2)),
            dma((others, 2)),
            V((groups, chips, rows, quarter), bf16),
            V((groups, chips, rows, quarter), bf16),
            V((groups, chips, rows, quarter), bf16),
            dma((groups, chips)),
            dma((groups, chips)),
            V((others, n * cap, quarter), bf16),
            V((others, n * cap, quarter), bf16),
            dma((n, others)),
            dma((n, others)),
            V((n * cap, quarter), bf16),
            V((n * cap, quarter), bf16),
            dma((n,)),
            dma((n,)),
            V((tokens, quarter), f32),
            V((tokens, 128), f32),
            V((tokens, width), bf16),
            V((1, width), f32),
            V(expert_ids.T.shape, jnp.int32),
            V(route_weight.T.shape, f32),
            V(conv_kernel.shape, f32),
            V((1, chan), f32),
            dma((6,)),
        ],
        compiler_params=pltpu.CompilerParams(
            collective_id=0, has_side_effects=True, vmem_limit_bytes=66_000_000
        ),
        name="block",
    )(
        moe_input,
        moe_gain.reshape(1, -1),
        expert_ids.T,
        route_weight.T,
        conv_kernel,
        ln_gain.reshape(1, -1),
        glu_value,
        glu_gate,
        out_weight,
        gate_weight,
        up_weight,
        down_weight,
    )
    return settle(
        pltpu.with_memory_space_constraint(mixed, pltpu.VMEM),
        pltpu.with_memory_space_constraint(routed, pltpu.VMEM),
    )


def settle_kernel(a_ref, b_ref, c_ref, d_ref, sem):
    first = pltpu.make_async_copy(a_ref, c_ref, sem.at[0])
    second = pltpu.make_async_copy(b_ref, d_ref, sem.at[1])
    first.start()
    second.start()
    first.wait()
    second.wait()


def settle(a, b):
    vmem = pl.BlockSpec(memory_space=pltpu.VMEM)
    hbm = pl.BlockSpec(memory_space=pltpu.HBM)
    return pl.pallas_call(
        settle_kernel,
        out_shape=(jax.ShapeDtypeStruct(a.shape, a.dtype), jax.ShapeDtypeStruct(b.shape, b.dtype)),
        in_specs=[vmem, vmem],
        out_specs=(hbm, hbm),
        scratch_shapes=[pltpu.SemaphoreType.DMA((2,))],
        name="settle",
    )(a, b)


def solution(mesh):
    in_specs = (
        P("ep", "tp"),
        P("ep", "tp"),
        P(None, "tp"),
        P("tp"),
        P("tp", None),
        P("ep", None),
        P(),
        P("ep", None, "tp"),
        P("ep", None, "tp"),
        P("ep", "tp", None),
        P("ep", None),
        P("ep", None),
    )
    out_specs = (P(("ep", "tp"), None), P("ep", "tp"))
    return jax.shard_map(
        on_device, mesh=mesh, in_specs=in_specs, out_specs=out_specs, check_vma=False
    )
```

```python
import functools
import types

import jax
import jax.numpy as jnp
from jax import lax
from jax.experimental import pallas as pl
from jax.experimental.pallas import tpu as pltpu
from jax.sharding import PartitionSpec as P

eps_rms = 1e-06
eps_norm = 1e-05
MESH = pl.DeviceIdType.MESH
f32 = jnp.float32
bf16 = jnp.bfloat16


def kernel(
    n,
    tp,
    cap,
    group,
    reach,
    moe_hbm,
    moe_gain_hbm,
    ids_t_hbm,
    route_t_hbm,
    taps_hbm,
    ln_gain_hbm,
    value_hbm,
    gate_hbm,
    w_out_hbm,
    w_gate_hbm,
    w_up_hbm,
    w_down_hbm,
    mixer_ref,
    expert_ref,
    value,
    gate,
    w_out,
    w_gate,
    w_up,
    w_down,
    load_sem,
    normed,
    slots,
    near_slots,
    onehots,
    arrived,
    near_send,
    near_recv,
    fn_send,
    fn_recv,
    a2a_send,
    a2a_recv,
    fx_send,
    fx_recv,
    fp_send,
    fp_recv,
    fq_send,
    fq_recv,
    gated,
    halo_in,
    halo_send,
    halo_recv,
    padded,
    conv,
    stat_out,
    stat_in,
    stat_send,
    stat_recv,
    act,
    mix_out,
    mix_own,
    mix_in,
    mix_send,
    mix_recv,
    mix_x_out,
    mix_x_in,
    mix_x_send,
    mix_x_recv,
    rs_out,
    rs_own,
    rs_in,
    rs_send,
    rs_recv,
    rx_out,
    rx_in,
    rx_send,
    rx_recv,
    answer,
    returned,
    ret_send,
    ret_recv,
    total,
    meta_ref,
    moe_ref,
    moe_gain_ref,
    ids_t_ref,
    route_t_ref,
    taps_ref,
    ln_gain_ref,
    small_sem,
):
    me = lax.axis_index("ep")
    mine = lax.axis_index("tp")
    core = lax.rem(mine, 2)
    chip = mine // 2
    partner = chip * 2 + 1 - core
    chips = tp // 2
    groups = n // group
    rows = group * cap
    tokens, width = moe_ref.shape
    quarter = width // tp
    length, chan = value.shape
    halo = halo_in.shape[0]
    own_rows = length // tp

    def toward(k):
        return lax.rem(me // 2 + k // 2, n // 2) * 2 + lax.rem(me + k, 2)

    def source(k):
        return lax.rem(me // 2 + n // 2 - k // 2, n // 2) * 2 + lax.rem(me + k, 2)

    def block(k):
        return pl.ds(pl.multiple_of(k * cap, cap), cap)

    def columns_of(part):
        return pl.ds(pl.multiple_of(part * quarter, 128), quarter)

    def across(j):
        there = lax.rem(chip + j, chips)
        here = lax.rem(chip + chips - j, chips)
        return there * 2 + core, here * 2 + core

    barrier = pltpu.get_barrier_semaphore()

    def greet_ep(k, _):
        pl.semaphore_signal(
            barrier, inc=1, device_id={"ep": lax.rem(me + k, n)}, device_id_type=MESH
        )
        return 0

    lax.fori_loop(1, n, greet_ep, 0)
    for j in range(1, tp):
        pl.semaphore_signal(
            barrier, inc=1, device_id={"tp": lax.rem(mine + j, tp)}, device_id_type=MESH
        )

    loads = [
        pltpu.make_async_copy(src, dst, load_sem.at[i])
        for i, (src, dst) in enumerate(
            [
                (value_hbm, value),
                (gate_hbm, gate),
                (w_out_hbm, w_out),
                (w_gate_hbm.at[0], w_gate),
                (w_up_hbm.at[0], w_up),
                (w_down_hbm.at[0], w_down),
            ]
        )
    ]
    smalls = [
        pltpu.make_async_copy(src, dst, small_sem.at[i])
        for i, (src, dst) in enumerate(
            [
                (moe_hbm, moe_ref),
                (moe_gain_hbm, moe_gain_ref),
                (ids_t_hbm, ids_t_ref),
                (route_t_hbm, route_t_ref),
                (taps_hbm, taps_ref),
                (ln_gain_hbm, ln_gain_ref),
            ]
        )
    ]
    for load in smalls:
        load.start()
    for load in loads:
        load.start()
    for load in smalls:
        load.wait()
    everything = moe_ref[...].astype(f32)
    inverse = lax.rsqrt(jnp.sum(everything * everything, axis=1, keepdims=True) / width + eps_rms)
    normed[...] = (everything * inverse * moe_gain_ref[...]).astype(bf16)
    lead = lax.broadcasted_iota(jnp.int32, (128, tokens), 0)
    meta = jnp.where(lead == 0, ids_t_ref[0:1, :].astype(f32), 0.0)
    meta = jnp.where(lead == 1, ids_t_ref[1:2, :].astype(f32), meta)
    meta = jnp.where(lead == 2, route_t_ref[0:1, :], meta)
    meta = jnp.where(lead == 3, route_t_ref[1:2, :], meta)
    meta_ref[...] = jnp.transpose(meta)
    row = lax.broadcasted_iota(jnp.int32, (tokens, tokens), 0)
    col = lax.broadcasted_iota(jnp.int32, (tokens, tokens), 1)
    below = (col < row).astype(f32).astype(bf16)
    above = (row < col).astype(f32).astype(bf16)

    def a2a_copy(k):
        return pltpu.make_async_remote_copy(
            src_ref=slots.at[block(k)],
            dst_ref=arrived.at[mine, block(k)],
            send_sem=a2a_send.at[k],
            recv_sem=a2a_recv.at[k],
            device_id={"ep": toward(k)},
            device_id_type=MESH,
        )

    def near_copy(xx):
        return pltpu.make_async_remote_copy(
            src_ref=near_slots.at[xx],
            dst_ref=arrived.at[xx * 2 + core, pl.ds(cap, cap)],
            send_sem=near_send.at[xx],
            recv_sem=near_recv.at[xx],
            device_id={"ep": toward(1)},
            device_id_type=MESH,
        )

    def slot_picks(k):
        expert = toward(k)
        member = jnp.maximum(
            (ids_t_ref[0:1, :] == expert).astype(f32), (ids_t_ref[1:2, :] == expert).astype(f32)
        )
        member = jnp.broadcast_to(member, (cap, tokens))
        place = jnp.dot(member.astype(bf16), above, preferred_element_type=f32)
        slot = lax.broadcasted_iota(jnp.int32, (cap, tokens), 0).astype(f32)
        return jnp.where(place == slot, member, 0.0).astype(bf16)

    def picked(pick, part):
        return jnp.dot(
            pick, normed[:, columns_of(part)], preferred_element_type=f32
        ).astype(bf16)

    pl.semaphore_wait(barrier, n - 1 + tp - 1)

    def dispatch(k, _):
        slots[block(k), :] = picked(slot_picks(k), mine)
        a2a_copy(k).start()
        return 0

    loads[0].wait()
    loads[1].wait()
    gated_now = (value[...].astype(f32) * jax.nn.sigmoid(gate[...].astype(f32))).astype(bf16)
    gated[...] = gated_now
    halo_copy = pltpu.make_async_remote_copy(
        src_ref=gated.at[pl.ds(length - halo, halo)],
        dst_ref=halo_in,
        send_sem=halo_send,
        recv_sem=halo_recv,
        device_id={"ep": lax.rem(me + 1, n)},
        device_id_type=MESH,
    )
    halo_copy.start()
    padded[pl.ds(halo, length), :] = gated_now.astype(f32)

    lax.fori_loop(2, n, dispatch, 0)
    pick = slot_picks(1)
    for xx in range(chips):
        near_slots[xx] = picked(pick, xx * 2 + core)
        near_copy(xx).start()

    pick = slot_picks(0)
    for part in range(tp):
        arrived[part, 0:cap, :] = picked(pick, part)

    def fx_copy(k, j):
        to, _ = across(j)
        return pltpu.make_async_remote_copy(
            src_ref=arrived.at[mine, block(k)],
            dst_ref=arrived.at[mine, block(k)],
            send_sem=fx_send.at[k, j - 1],
            recv_sem=fx_recv.at[k, j - 1],
            device_id={"tp": to},
            device_id_type=MESH,
        )

    def fp_copy(k):
        return pltpu.make_async_remote_copy(
            src_ref=arrived.at[mine, block(k)],
            dst_ref=arrived.at[mine, block(k)],
            send_sem=fp_send.at[k],
            recv_sem=fp_recv.at[k],
            device_id={"tp": partner},
            device_id_type=MESH,
        )

    def fq_copy(k, j):
        _, origin = across(j)
        return pltpu.make_async_remote_copy(
            src_ref=arrived.at[origin, block(k)],
            dst_ref=arrived.at[origin, block(k)],
            send_sem=fq_send.at[k, j - 1],
            recv_sem=fq_recv.at[k, j - 1],
            device_id={"tp": partner},
            device_id_type=MESH,
        )

    def fn_copy(xx):
        return pltpu.make_async_remote_copy(
            src_ref=arrived.at[xx * 2 + core, pl.ds(cap, cap)],
            dst_ref=arrived.at[xx * 2 + core, pl.ds(cap, cap)],
            send_sem=fn_send.at[xx],
            recv_sem=fn_recv.at[xx],
            device_id={"tp": partner},
            device_id_type=MESH,
        )

    def over_group(g, do, first=2):
        def one(k, _):
            @pl.when(k >= first)
            def _():
                do(k)

            return 0

        lax.fori_loop(g * group, (g + 1) * group, one, 0)

    def forward_first(g):
        def one(k):
            a2a_copy(k).wait_recv()
            for j in range(1, chips):
                fx_copy(k, j).start()
            fp_copy(k).start()

        over_group(g, one)

    def forward_second(g):
        def one(k):
            for j in range(1, chips):
                fx_copy(k, j).wait_recv()
                fq_copy(k, j).start()

        over_group(g, one)

    def forward_near():
        for xx in range(chips):
            near_copy(xx).wait_recv()
            fn_copy(xx).start()

    halo_copy.wait_recv()
    padded[pl.ds(0, halo), :] = jnp.where(me == 0, 0.0, halo_in[...].astype(f32))
    step_rows = 64
    window = step_rows + halo

    for lane in range(0, chan, 128):

        def conv_step(i, _):
            base = pl.multiple_of(i * step_rows, step_rows)
            rows_in = padded[pl.ds(base, window), lane : lane + 128]
            result = jnp.zeros((step_rows, 128), f32)
            for shift in range(8):
                turned = rows_in if shift == 0 else pltpu.roll(rows_in, window - shift, 0)
                for tap in range(reach):
                    offset = halo - tap
                    if offset % 8 == shift:
                        begin = offset - shift
                        result = (
                            result
                            + taps_ref[tap : tap + 1, lane : lane + 128]
                            * turned[begin : begin + step_rows]
                        )
            conv[pl.ds(base, step_rows), lane : lane + 128] = result
            return 0

        lax.fori_loop(0, length // step_rows, conv_step, 0)

    convolved = conv[...]
    sums = jnp.sum(convolved, axis=1, keepdims=True)
    squares = jnp.sum(convolved * convolved, axis=1, keepdims=True)
    lanes = lax.broadcasted_iota(jnp.int32, (length, 128), 1)
    packed = jnp.where(lanes == 0, sums, jnp.where(lanes == 1, squares, 0.0))
    stat_out[...] = jnp.transpose(packed)[0:8]

    def stat_copy(j):
        return pltpu.make_async_remote_copy(
            src_ref=stat_out,
            dst_ref=stat_in.at[j - 1],
            send_sem=stat_send.at[j - 1],
            recv_sem=stat_recv.at[j - 1],
            device_id={"tp": lax.rem(mine + j, tp)},
            device_id_type=MESH,
        )

    for j in range(1, tp):
        stat_copy(j).start()

    forward_near()
    forward_first(0)
    if groups > 1:
        forward_first(1)
    forward_second(0)

    stats = stat_out[...]
    for j in range(1, tp):
        stat_copy(j).wait_recv()
        stats = stats + stat_in[j - 1]
    stats = jnp.concatenate([stats, jnp.zeros((120, length), f32)], axis=0)
    columns = jnp.transpose(stats)
    mean = columns[:, 0:1] / (chan * tp)
    variance = columns[:, 1:2] / (chan * tp) - mean * mean
    scaled = (conv[...] - mean) * lax.rsqrt(variance + eps_norm) * ln_gain_ref[...]
    act[...] = jax.nn.silu(scaled).astype(bf16)

    def mix_copy(xx):
        return pltpu.make_async_remote_copy(
            src_ref=mix_out.at[xx],
            dst_ref=mix_in.at[xx],
            send_sem=mix_send.at[xx],
            recv_sem=mix_recv.at[xx],
            device_id={"tp": partner},
            device_id_type=MESH,
        )

    def mix_part(owner):
        begin = pl.multiple_of(owner * own_rows, own_rows)
        return jnp.dot(act[pl.ds(begin, own_rows), :], w_out[...], preferred_element_type=f32)

    loads[2].wait()

    def mix_first(xx, _):
        mix_out[xx] = mix_part(xx * 2 + 1 - core).astype(bf16)
        mix_copy(xx).start()
        return 0

    def mix_second(xx, _):
        mix_own[xx] = mix_part(xx * 2 + core).astype(bf16)
        return 0

    lax.fori_loop(0, chips, mix_first, 0)
    lax.fori_loop(0, chips, mix_second, 0)

    half = own_rows // 2

    def mix_x_copy(j, part):
        to, _ = across(j)
        span = pl.ds(part * half, half)
        return pltpu.make_async_remote_copy(
            src_ref=mix_x_out.at[j - 1, span],
            dst_ref=mix_x_in.at[j - 1, span],
            send_sem=mix_x_send.at[j - 1, part],
            recv_sem=mix_x_recv.at[j - 1, part],
            device_id={"tp": to},
            device_id_type=MESH,
        )

    def mix_stage():
        for xx in range(chips):
            mix_copy(xx).wait_recv()
        for j in range(1, chips):
            there = lax.rem(chip + j, chips)
            mix_x_out[j - 1] = (mix_own[there].astype(f32) + mix_in[there].astype(f32)).astype(
                bf16
            )
    loads[3].wait()
    loads[4].wait()
    loads[5].wait()

    def rs_copy(g, xx):
        return pltpu.make_async_remote_copy(
            src_ref=rs_out.at[g, xx],
            dst_ref=rs_in.at[g, xx],
            send_sem=rs_send.at[g, xx],
            recv_sem=rs_recv.at[g, xx],
            device_id={"tp": partner},
            device_id_type=MESH,
        )

    def rx_copy(k, j):
        to, _ = across(j)
        return pltpu.make_async_remote_copy(
            src_ref=rx_out.at[j - 1, block(k)],
            dst_ref=rx_in.at[j - 1, block(k)],
            send_sem=rx_send.at[k, j - 1],
            recv_sem=rx_recv.at[k, j - 1],
            device_id={"tp": to},
            device_id_type=MESH,
        )

    def ret_copy(k):
        return pltpu.make_async_remote_copy(
            src_ref=answer.at[block(k)],
            dst_ref=returned.at[block(k)],
            send_sem=ret_send.at[k],
            recv_sem=ret_recv.at[k],
            device_id={"ep": source(k)},
            device_id_type=MESH,
        )

    def expert_step(g):
        @pl.when(g == 0)
        def _():
            for xx in range(chips):
                fn_copy(xx).wait_recv()

        def one(k):
            fp_copy(k).wait_recv()
            for j in range(1, chips):
                fq_copy(k, j).wait_recv()

        over_group(g, one)
        span = pl.ds(pl.multiple_of(g * rows, rows), rows)
        x = jnp.concatenate([arrived[part, span] for part in range(tp)], axis=1)
        gate_act = jnp.dot(x, w_gate[...], preferred_element_type=f32)
        up_act = jnp.dot(x, w_up[...], preferred_element_type=f32)
        hidden = (jax.nn.silu(gate_act) * up_act).astype(bf16)
        for xx in range(chips):
            begin = pl.multiple_of((xx * 2 + 1 - core) * quarter, 128)
            rs_out[g, xx] = jnp.dot(
                hidden, w_down[:, pl.ds(begin, quarter)], preferred_element_type=f32
            ).astype(bf16)
            rs_copy(g, xx).start()
        for xx in range(chips):
            begin = pl.multiple_of((xx * 2 + core) * quarter, 128)
            rs_own[g, xx] = jnp.dot(
                hidden, w_down[:, pl.ds(begin, quarter)], preferred_element_type=f32
            ).astype(bf16)

    def sum_step(g):
        for xx in range(chips):
            rs_copy(g, xx).wait_recv()
        span = pl.ds(pl.multiple_of(g * rows, rows), rows)
        for j in range(1, chips):
            there = lax.rem(chip + j, chips)
            rx_out[j - 1, span] = (
                rs_own[g, there].astype(f32) + rs_in[g, there].astype(f32)
            ).astype(bf16)

        def one(k):
            for j in range(1, chips):
                rx_copy(k, j).start()

        over_group(g, one, 0)

    def return_step(g):
        def one(k):
            inner = pl.ds(pl.multiple_of((k - g * group) * cap, cap), cap)
            result = rs_own[g, chip, inner].astype(f32) + rs_in[g, chip, inner].astype(f32)
            for j in range(1, chips):
                rx_copy(k, j).wait_recv()
                result = result + rx_in[j - 1, block(k)].astype(f32)
            answer[block(k), :] = result.astype(bf16)

            @pl.when(k > 0)
            def _():
                ret_copy(k).start()

        over_group(g, one, 0)

    total[...] = jnp.zeros_like(total)

    def combine_step(g):
        def take(k, _):
            @pl.when(k > 0)
            def _():
                ret_copy(k).wait_recv()

            expert = toward(k)
            weight = jnp.where(meta_ref[:, 0:1] == expert.astype(f32), meta_ref[:, 2:3], 0.0) + jnp.where(
                meta_ref[:, 1:2] == expert.astype(f32), meta_ref[:, 3:4], 0.0
            )
            answers = returned[block(k), :]
            total[...] += weight * jnp.dot(onehots[k], answers, preferred_element_type=f32)
            return 0

        lax.fori_loop(g * group, (g + 1) * group, take, 0)

    def place_of(k, _):
        expert = toward(k)
        member = jnp.maximum(
            (meta_ref[:, 0:1] == expert.astype(f32)).astype(f32), (meta_ref[:, 1:2] == expert.astype(f32)).astype(f32)
        )
        member = jnp.broadcast_to(member, (tokens, cap))
        place = jnp.dot(below, member.astype(bf16), preferred_element_type=f32)
        slot = lax.broadcasted_iota(jnp.int32, (tokens, cap), 1).astype(f32)
        onehots[k] = jnp.where(place == slot, member, 0.0).astype(bf16)
        return 0

    def step(g, _):
        @pl.when(g < groups)
        def _():
            expert_step(g)

        @pl.when(g < groups)
        def _():
            sum_step(g)

        @pl.when(g + 1 < groups)
        def _():
            forward_second(g + 1)

        @pl.when(g == groups)
        def _():
            lax.fori_loop(0, n, place_of, 0)

        @pl.when((g >= 1) & (g < groups + 1))
        def _():
            return_step(g - 1)

        @pl.when(g == 0)
        def _():
            mix_stage()

        @pl.when(g + 2 < groups)
        def _():
            forward_first(g + 2)

        @pl.when(g == groups - 1)
        def _():
            for j in range(1, chips):
                mix_x_copy(j, 0).start()
                mix_x_copy(j, 1).start()

        return 0

    lax.fori_loop(0, groups + 1, step, 0)
    returned[0:cap, :] = answer[0:cap, :]

    def combine(g, _):
        combine_step(g)
        return 0

    lax.fori_loop(0, groups, combine, 0)
    expert_ref[...] = total[...].astype(bf16)

    mixed = mix_own[chip].astype(f32) + mix_in[chip].astype(f32)
    for j in range(1, chips):
        mix_x_copy(j, 0).wait_recv()
        mix_x_copy(j, 1).wait_recv()
        mixed = mixed + mix_x_in[j - 1].astype(f32)
    mixer_ref[...] = mixed.astype(bf16)

    ret_copy(1).wait_send()

    def left(k, _):
        a2a_copy(k).wait_send()
        ret_copy(k).wait_send()
        fp_copy(k).wait_send()
        for j in range(1, chips):
            fx_copy(k, j).wait_send()
            fq_copy(k, j).wait_send()
        return 0

    lax.fori_loop(2, n, left, 0)

    def left_x(k, _):
        for j in range(1, chips):
            rx_copy(k, j).wait_send()
        return 0

    lax.fori_loop(0, n, left_x, 0)
    halo_copy.wait_send()
    for j in range(1, tp):
        stat_copy(j).wait_send()
    for xx in range(chips):
        mix_copy(xx).wait_send()
        near_copy(xx).wait_send()
        fn_copy(xx).wait_send()
    for j in range(1, chips):
        mix_x_copy(j, 0).wait_send()
        mix_x_copy(j, 1).wait_send()

    def left_group(g, _):
        for xx in range(chips):
            rs_copy(g, xx).wait_send()
        return 0

    lax.fori_loop(0, groups, left_group, 0)


def line_kernel(n, tp, cap, reach, near, names, *refs):
    r = types.SimpleNamespace(**dict(zip(names, refs)))
    me = lax.axis_index("ep")
    mine = lax.axis_index("tp")
    core = lax.rem(mine, 2)
    chip = mine // 2
    partner = chip * 2 + 1 - core
    across = (1 - chip) * 2 + core
    stations = n // 2
    z = me // 2
    y = lax.rem(me, 2)
    beside = z * 2 + 1 - y
    tokens, width = r.moe.shape
    quarter = width // tp
    length, chan = r.value.shape
    halo = r.halo_in.shape[0]
    own_rows = length // tp
    behind = jnp.minimum(z, stations - 1 - z)
    inner = behind >= 1
    longer = jnp.where(stations - 1 - z > z, 1, -1)

    def distance(j):
        return jnp.where(j <= 2 * behind, (j + 1) // 2, j - behind)

    def origin(j):
        turn = jnp.where((j <= 2 * behind) & (lax.rem(j, 2) == 1), -longer, longer)
        return z + turn * distance(j)

    def home(s):
        return origin(s // 2) * 2 + lax.rem(y + s, 2)

    def block(k):
        return pl.ds(pl.multiple_of(k * cap, cap), cap)

    def remote(src, dst, send, recv, **device):
        return pltpu.make_async_remote_copy(
            src_ref=src,
            dst_ref=dst,
            send_sem=send,
            recv_sem=recv,
            device_id=device,
            device_id_type=MESH,
        )

    barrier = pltpu.get_barrier_semaphore()

    def greet_ep(k, _):
        pl.semaphore_signal(
            barrier, inc=1, device_id={"ep": lax.rem(me + k, n)}, device_id_type=MESH
        )
        return 0

    lax.fori_loop(1, n, greet_ep, 0)
    for j in range(1, tp):
        pl.semaphore_signal(
            barrier, inc=1, device_id={"tp": lax.rem(mine + j, tp)}, device_id_type=MESH
        )

    loads = {
        name: pltpu.make_async_copy(src, dst, r.load_sem.at[i])
        for i, (name, src, dst) in enumerate(
            [
                ("moe", r.moe_hbm, r.moe),
                ("moe_gain", r.moe_gain_hbm, r.moe_gain),
                ("ids", r.ids_hbm, r.ids),
                ("route", r.route_hbm, r.route),
                ("value", r.value_hbm, r.value),
                ("gate", r.gate_hbm, r.gate),
                ("taps", r.taps_hbm, r.taps),
                ("ln_gain", r.ln_gain_hbm, r.ln_gain),
                ("w_gate", r.w_gate_hbm.at[0], r.w_gate),
                ("w_up", r.w_up_hbm.at[0], r.w_up),
                ("w_down", r.w_down_hbm.at[0], r.w_down),
                ("w_out", r.w_out_hbm, r.w_out),
            ]
        )
    }
    late = ("w_gate", "w_up", "w_down", "w_out")
    for name, load in loads.items():
        if name not in late:
            load.start()

    def own_copy(up, xx):
        return remote(
            r.normed.at[xx * 2 + core],
            r.tok.at[z, xx],
            r.own_send.at[up, xx],
            r.tok_recv.at[z, xx],
            ep=(z + 2 * up - 1) * 2 + y,
        )

    def own_ids(up):
        return remote(
            r.ids_all.at[z],
            r.ids_all.at[z],
            r.ids_own_send.at[up],
            r.ids_recv.at[z],
            ep=(z + 2 * up - 1) * 2 + y,
        )

    def onward(zz):
        return jnp.where(zz < z, z + 1, z - 1)

    def pass_copy(zz, xx):
        return remote(
            r.tok.at[zz, xx],
            r.tok.at[zz, xx],
            r.pass_send.at[zz, xx],
            r.tok_recv.at[zz, xx],
            ep=onward(zz) * 2 + y,
        )

    def pass_ids(zz):
        return remote(
            r.ids_all.at[zz],
            r.ids_all.at[zz],
            r.ids_pass_send.at[zz],
            r.ids_recv.at[zz],
            ep=onward(zz) * 2 + y,
        )

    def side_copy(j, xx):
        return remote(
            r.side.at[j, xx],
            r.arrived.at[xx * 2 + core, block(2 * j + 1)],
            r.side_send.at[j, xx],
            r.side_recv.at[j, xx],
            ep=beside,
        )

    def slant_copy(j):
        return remote(
            r.side.at[j, chip],
            r.arrived.at[mine, block(2 * j + 1)],
            r.slant_send.at[j],
            r.side_recv.at[j, chip],
            ep=beside,
            tp=across,
        )

    def core_copy(s, xx):
        return remote(
            r.arrived.at[xx * 2 + core, block(s)],
            r.arrived.at[xx * 2 + core, block(s)],
            r.core_send.at[s, xx],
            r.core_recv.at[s, xx],
            tp=partner,
        )

    def cross_copy(s):
        return remote(
            r.arrived.at[mine, block(s)],
            r.arrived.at[mine, block(s)],
            r.cross_send.at[s],
            r.cross_recv.at[s],
            tp=across,
        )

    def rs_copy(s, xx):
        return remote(
            r.rs_out.at[s, xx], r.rs_in.at[s, xx], r.rs_send.at[s, xx], r.rs_recv.at[s, xx], tp=partner
        )

    def rx_copy(s):
        return remote(r.rx_out.at[s], r.rx_in.at[s], r.rx_send.at[s], r.rx_recv.at[s], tp=across)

    def ret_copy(s):
        return remote(
            r.answer.at[s], r.returned.at[me], r.ret_send.at[s], r.ret_recv.at[me], ep=home(s)
        )

    def ret_arrival(s):
        there = home(s)
        return remote(
            r.answer.at[s], r.returned.at[there], r.ret_send.at[s], r.ret_recv.at[there], ep=there
        )

    halo_copy = remote(
        r.gated.at[pl.ds(length - halo, halo)],
        r.halo_in,
        r.halo_send,
        r.halo_recv,
        ep=lax.rem(me + 1, n),
    )

    def stat_copy(j):
        return remote(
            r.stat_out,
            r.stat_in.at[j - 1],
            r.stat_send.at[j - 1],
            r.stat_recv.at[j - 1],
            tp=lax.rem(mine + j, tp),
        )

    def mix_copy(xx):
        return remote(r.mix_out.at[xx], r.mix_in.at[xx], r.mix_send.at[xx], r.mix_recv.at[xx], tp=partner)

    pieces = r.mix_x_send.shape[0]
    piece = own_rows // pieces

    def mix_x_copy(part):
        span = pl.ds(pl.multiple_of(part * piece, piece), piece)
        return remote(
            r.mix_x_out.at[span], r.mix_x_in.at[span], r.mix_x_send.at[part], r.mix_x_recv.at[part], tp=across
        )

    loads["moe"].wait()
    loads["moe_gain"].wait()
    everything = r.moe[...].astype(f32)
    inverse = lax.rsqrt(jnp.sum(everything * everything, axis=1, keepdims=True) / width + eps_rms)
    normed_now = (everything * inverse * r.moe_gain[...]).astype(bf16)
    for part in range(tp):
        r.normed[part] = normed_now[:, part * quarter : (part + 1) * quarter]
    loads["ids"].wait()
    loads["route"].wait()
    r.ids_all[z] = jnp.concatenate([r.ids[...].astype(f32), jnp.zeros((6, tokens), f32)], axis=0)
    for name in late:
        loads[name].start()
    loads["value"].wait()
    loads["gate"].wait()
    gated_now = (r.value[...].astype(f32) * jax.nn.sigmoid(r.gate[...].astype(f32))).astype(bf16)
    r.gated[...] = gated_now
    r.padded[pl.ds(halo, length), :] = gated_now.astype(f32)

    pl.semaphore_wait(barrier, n - 1 + tp - 1)
    halo_copy.start()

    def each_way(do):
        @pl.when(z > 0)
        def _():
            do(0)

        @pl.when(z < stations - 1)
        def _():
            do(1)

    each_way(lambda up: own_ids(up).start())
    each_way(lambda up: own_copy(up, chip).start())
    if near > 1:
        each_way(lambda up: own_copy(up, 1 - chip).start())

    row = lax.broadcasted_iota(jnp.int32, (tokens, tokens), 0)
    col = lax.broadcasted_iota(jnp.int32, (tokens, tokens), 1)
    r.above[...] = (row < col).astype(f32).astype(bf16)
    slot_rows = lax.broadcasted_iota(jnp.int32, (cap, tokens), 0).astype(f32)

    def choices(zz):
        here = (z * 2 + lax.rem(y + lax.broadcasted_iota(jnp.int32, (16, tokens), 0), 2)).astype(f32)
        chosen = r.ids_all[zz]
        member = jnp.maximum(
            (chosen[0:1, :] == here).astype(f32), (chosen[1:2, :] == here).astype(f32)
        )
        place = jnp.dot(member.astype(bf16), r.above[...], preferred_element_type=f32)
        key = jnp.where(member > 0.0, place, -1.0)
        ours = (slot_rows == key[0:1, :]).astype(f32).astype(bf16)
        theirs = (slot_rows == key[1:2, :]).astype(f32).astype(bf16)
        return ours, theirs

    ours, theirs = choices(z)
    for xx in (chip, 1 - chip):
        r.side[0, xx] = jnp.dot(
            theirs, r.normed[xx * 2 + core], preferred_element_type=f32
        ).astype(bf16)
        side_copy(0, xx).start()
    for part in range(tp):
        r.arrived[part, block(0), :] = jnp.dot(
            ours, r.normed[part], preferred_element_type=f32
        ).astype(bf16)

    def expert_step(s, first=False):
        def partial(part):
            rows = pl.ds(pl.multiple_of(part * quarter, quarter), quarter)
            x = r.arrived[part, block(s)]
            return (
                jnp.dot(x, r.w_gate[rows, :], preferred_element_type=f32),
                jnp.dot(x, r.w_up[rows, :], preferred_element_type=f32),
            )

        gate_act, up_act = partial(core)
        more = partial(2 + core)
        gate_act, up_act = gate_act + more[0], up_act + more[1]
        for xx in range(2):
            if not first:
                core_copy(s, xx).wait_recv()
            more = partial(xx * 2 + 1 - core)
            gate_act, up_act = gate_act + more[0], up_act + more[1]
        hidden = (jax.nn.silu(gate_act) * up_act).astype(bf16)
        for xx in (1 - chip, chip):
            begin = pl.multiple_of((xx * 2 + 1 - core) * quarter, 128)
            r.rs_out[s, xx] = jnp.dot(
                hidden, r.w_down[:, pl.ds(begin, quarter)], preferred_element_type=f32
            ).astype(bf16)
            rs_copy(s, xx).start()
        for xx in (1 - chip, chip):
            begin = pl.multiple_of((xx * 2 + core) * quarter, 128)
            r.rs_own[s, xx] = jnp.dot(
                hidden, r.w_down[:, pl.ds(begin, quarter)], preferred_element_type=f32
            ).astype(bf16)

    def sum_step(s):
        rs_copy(s, 1 - chip).wait_recv()
        r.rx_out[s] = (r.rs_own[s, 1 - chip].astype(f32) + r.rs_in[s, 1 - chip].astype(f32)).astype(bf16)
        rx_copy(s).start()

    def return_step(s):
        rs_copy(s, chip).wait_recv()
        rx_copy(s).wait_recv()
        result = r.rs_own[s, chip].astype(f32) + r.rs_in[s, chip].astype(f32)
        r.answer[s] = (result + r.rx_in[s].astype(f32)).astype(bf16)

        @pl.when(s > 0)
        def _():
            ret_copy(s).start()

    loads["taps"].wait()
    step_rows = 64
    window = step_rows + halo

    def conv_rows(lane, begin, end):
        def conv_step(i, _):
            base = pl.multiple_of(i * step_rows, step_rows)
            rows_in = r.padded[pl.ds(base, window), lane : lane + 128]
            result = jnp.zeros((step_rows, 128), f32)
            for shift in range(8):
                turned = rows_in if shift == 0 else pltpu.roll(rows_in, window - shift, 0)
                for tap in range(reach):
                    offset = halo - tap
                    if offset % 8 == shift:
                        begin = offset - shift
                        result = (
                            result
                            + r.taps[tap : tap + 1, lane : lane + 128]
                            * turned[begin : begin + step_rows]
                        )
            r.conv[pl.ds(base, step_rows), lane : lane + 128] = result
            return 0

        lax.fori_loop(begin, end, conv_step, 0)

    for lane in range(0, chan, 128):
        conv_rows(lane, 1, length // step_rows)
    lead = lax.broadcasted_iota(jnp.int32, (128, tokens), 0)
    meta = jnp.where(lead == 0, r.ids[0:1, :].astype(f32), 0.0)
    meta = jnp.where(lead == 1, r.ids[1:2, :].astype(f32), meta)
    meta = jnp.where(lead == 2, r.route[0:1, :], meta)
    meta = jnp.where(lead == 3, r.route[1:2, :], meta)
    meta = jnp.transpose(meta)
    order = lax.broadcasted_iota(jnp.int32, (tokens, 128), 1)
    expert = home(order).astype(f32)
    first = (meta[:, 0:1] == expert) & (order < n)
    second = (meta[:, 1:2] == expert) & (order < n)
    member = jnp.maximum(first.astype(f32), second.astype(f32))
    below = (col < row).astype(f32).astype(bf16)
    place = jnp.dot(below, member.astype(bf16), preferred_element_type=f32)
    key = jnp.where(member > 0.0, place, -1.0)
    weights = jnp.where(first, meta[:, 2:3], 0.0) + jnp.where(second, meta[:, 3:4], 0.0)
    r.key[...] = key
    r.weights[...] = weights
    halo_copy.wait_recv()
    r.padded[pl.ds(0, halo), :] = jnp.where(me == 0, 0.0, r.halo_in[...].astype(f32))
    for lane in range(0, chan, 128):
        conv_rows(lane, 0, 1)

    convolved = r.conv[...]
    sums = jnp.sum(convolved, axis=1, keepdims=True)
    squares = jnp.sum(convolved * convolved, axis=1, keepdims=True)
    lanes = lax.broadcasted_iota(jnp.int32, (length, 128), 1)
    packed = jnp.where(lanes == 0, sums, jnp.where(lanes == 1, squares, 0.0))
    r.stat_out[...] = jnp.transpose(packed)[0:8]
    for j in range(1, tp):
        stat_copy(j).start()

    loads["w_gate"].wait()
    loads["w_up"].wait()
    loads["w_down"].wait()
    expert_step(0, first=True)

    loads["ln_gain"].wait()
    loads["w_out"].wait()
    sum_step(0)
    stats = r.stat_out[...]
    for j in range(1, tp):
        stat_copy(j).wait_recv()
        stats = stats + r.stat_in[j - 1]
    stats = jnp.concatenate([stats, jnp.zeros((120, length), f32)], axis=0)
    columns = jnp.transpose(stats)
    mean = columns[:, 0:1] / (chan * tp)
    variance = columns[:, 1:2] / (chan * tp) - mean * mean
    scaled = (r.conv[...] - mean) * lax.rsqrt(variance + eps_norm) * r.ln_gain[...]
    r.act[...] = jax.nn.silu(scaled).astype(bf16)

    def mix_part(owner):
        begin = pl.multiple_of(owner * own_rows, own_rows)
        return jnp.dot(r.act[pl.ds(begin, own_rows), :], r.w_out[...], preferred_element_type=f32)

    for xx in (1 - chip, chip):
        r.mix_out[xx] = mix_part(xx * 2 + 1 - core).astype(bf16)
        mix_copy(xx).start()
        r.mix_own[xx] = mix_part(xx * 2 + core).astype(bf16)
    mix_copy(1 - chip).wait_recv()
    for part in range(pieces):
        span = pl.ds(part * piece, piece)
        r.mix_x_out[span] = (
            r.mix_own[1 - chip, span].astype(f32) + r.mix_in[1 - chip, span].astype(f32)
        ).astype(bf16)
    mix_x_copy(0).start()

    def pull(j):
        zz = origin(j)
        there = onward(zz)
        pass_ids(zz).wait_recv()
        pass_copy(zz, chip).wait_recv()

        @pl.when((there >= 0) & (there < stations))
        def _():
            pass_ids(zz).start()
            pass_copy(zz, chip).start()

    def pull_rest(j):
        zz = origin(j)
        there = onward(zz)
        pass_copy(zz, 1 - chip).wait_recv()

        @pl.when((there >= 0) & (there < stations) & (distance(j) + 1 < near))
        def _():
            pass_copy(zz, 1 - chip).start()

    def absorb(j):
        zz = origin(j)
        full = distance(j) < near

        @pl.when(full)
        def _():
            pull_rest(j)

        ours, theirs = choices(zz)
        both = jnp.concatenate([ours, theirs], axis=0)

        def spread(xx):
            rows = jnp.dot(both, r.tok[zz, xx], preferred_element_type=f32).astype(bf16)
            r.side[j, xx] = rows[cap:]
            r.arrived[xx * 2 + core, block(2 * j), :] = rows[:cap]
            side_copy(j, xx).start()

            @pl.when(jnp.logical_not(full))
            def _():
                cross_copy(2 * j).start()
                slant_copy(j).start()

            core_copy(2 * j, xx).start()

        spread(chip)

        @pl.when(full)
        def _():
            spread(1 - chip)

    def gather_side(j):
        for xx in (chip, 1 - chip):
            side_copy(j, xx).wait_recv()
            core_copy(2 * j + 1, xx).start()

    def gather_cross(s):
        @pl.when((distance(s // 2) >= near) & (lax.rem(s, 2) == 0))
        def _():
            cross_copy(s).wait_recv()
            core_copy(s, 1 - chip).start()

    @pl.when(inner)
    def _():
        pull(1)
        pull(2)

    plan = schedule(stations)
    early = min(pieces - 1, 2)

    def entry(name, i):
        found = jnp.int32(-1)
        for k, (end, mid) in enumerate(plan[name]):
            found = jnp.where(i == k, jnp.where(inner, mid, end), found)
        return found

    def step(i, _):
        a = entry("arrive", i)
        e = entry("expert", i)
        b = entry("answer", i)
        c = entry("pull", i)
        d = entry("sum", i)
        j = a // 2

        @pl.when(c >= 0)
        def _():
            pull(c)

        @pl.when((a >= 0) & (lax.rem(a, 2) == 0))
        def _():
            @pl.when(jnp.logical_not(inner))
            def _():
                pull(j)

            absorb(j)

        @pl.when((a >= 0) & (lax.rem(a, 2) == 1))
        def _():
            gather_side(j)

        @pl.when(e >= 0)
        def _():
            gather_cross(e)
            expert_step(e)

        @pl.when(b >= 0)
        def _():
            return_step(b)

        @pl.when(d >= 0)
        def _():
            sum_step(d)

        @pl.when((i + 1 <= early) & jnp.logical_not(inner))
        def _():
            mix_x_copy(i + 1).start()

        return 0

    lax.fori_loop(0, len(plan["arrive"]), step, 0)

    slot_columns = lax.broadcasted_iota(jnp.int32, (tokens, cap), 1).astype(f32)

    def take(s):
        onehot = (r.key[:, s : s + 1] == slot_columns).astype(f32).astype(bf16)
        if s > 0:
            ret_arrival(s).wait_recv()
            rows = r.returned[home(s)]
        else:
            rows = r.answer[0]
        return r.weights[:, s : s + 1] * jnp.dot(onehot, rows, preferred_element_type=f32)

    for part in range(1, pieces):
        if part > early:
            mix_x_copy(part).start()
        else:

            @pl.when(inner)
            def _():
                mix_x_copy(part).start()

    for k in range(len(plan["finish"])):
        b = jnp.where(inner, *reversed(plan["finish"][k]))

        @pl.when(b >= 0)
        def _():
            return_step(b)

        if k == 0:
            r.total[...] = take(0)
        elif k == 1:
            r.total[...] += take(1)

    mix_copy(chip).wait_recv()
    mixed = r.mix_own[chip].astype(f32) + r.mix_in[chip].astype(f32)
    for part in range(pieces):
        mix_x_copy(part).wait_recv()
    r.mixer_out[...] = (mixed + r.mix_x_in[...].astype(f32)).astype(bf16)
    for s in range(2, n - 1):
        r.total[...] += take(s)
    r.expert_out[...] = (r.total[...] + take(n - 1)).astype(bf16)

    each_way(lambda up: own_ids(up).wait_send())
    each_way(lambda up: own_copy(up, chip).wait_send())
    if near > 1:
        each_way(lambda up: own_copy(up, 1 - chip).wait_send())

    def left(j, _):
        zz = origin(j)
        there = onward(zz)
        full = distance(j) < near

        @pl.when((there >= 0) & (there < stations))
        def _():
            pass_ids(zz).wait_send()
            pass_copy(zz, chip).wait_send()

            @pl.when(distance(j) + 1 < near)
            def _():
                pass_copy(zz, 1 - chip).wait_send()

        side_copy(j, chip).wait_send()

        @pl.when(full)
        def _():
            side_copy(j, 1 - chip).wait_send()

        for s in (2 * j, 2 * j + 1):
            for xx in range(2):
                core_copy(s, xx).wait_send()

        @pl.when(jnp.logical_not(full))
        def _():
            cross_copy(2 * j).wait_send()
            slant_copy(j).wait_send()

        return 0

    lax.fori_loop(1, stations, left, 0)
    for xx in range(2):
        side_copy(0, xx).wait_send()
        core_copy(1, xx).wait_send()
        mix_copy(xx).wait_send()

    def left_more(s, _):
        for xx in range(2):
            rs_copy(s, xx).wait_send()
        rx_copy(s).wait_send()

        @pl.when(s > 0)
        def _():
            ret_copy(s).wait_send()

        return 0

    lax.fori_loop(0, n, left_more, 0)
    halo_copy.wait_send()
    for j in range(1, tp):
        stat_copy(j).wait_send()
    for part in range(pieces):
        mix_x_copy(part).wait_send()


def schedule(stations):
    total = 2 * stations
    if stations == 4:
        ends = dict(
            arrive=[1, 2, 3, 4, 6, 5, -1, 7],
            expert=[1, 2, 3, 4, -1, 5, 6, 7],
            sum=[1, 2, 3, -1, 4, 5, 6, 7],
            answer=[-1, 0, 1, 2, -1, 3, -1, 4],
            finish=[5, 6, 7],
        )
        mids = dict(
            arrive=[1, 2, 4, 3, 6, 5, 7],
            expert=[1, 2, 4, 3, 6, 5, 7],
            answer=[-1, 0, -1, -1, 4, 1, 6],
            sum=[1, 2, 4, 3, 6, 5, 7],
            pull=[-1, -1, -1, 3],
            finish=[2, 5, 3, 7],
        )
    else:
        arrive = [1] + list(range(2, total, 2)) + list(range(3, total, 2))
        ends = dict(arrive=arrive, expert=[1] + [-1] * (total - 2) + list(range(2, total)))
        ends["finish"] = list(range(total))
        ends["sum"] = ends["expert"]
        mids = dict(ends, pull=[-1] + list(range(3, stations)))
    plan = {}
    steps = max(len(part) for part in list(ends.values()) + list(mids.values()))
    for name in ("arrive", "expert", "sum", "answer", "pull", "finish"):
        one, two = ends.get(name, []), mids.get(name, [])
        used = max(len(one), len(two)) if name == "finish" else steps
        plan[name] = [tuple((part + [-1] * used)[k] for part in (one, two)) for k in range(used)]
    return plan


def line_call(
    near,
    glu_value,
    glu_gate,
    conv_kernel,
    ln_gain,
    out_weight,
    moe_input,
    moe_gain,
    gate_weight,
    up_weight,
    down_weight,
    expert_ids,
    route_weight,
):
    n = lax.axis_size("ep")
    tp = lax.axis_size("tp")
    stations = n // 2
    length, chan = glu_value.shape
    reach = conv_kernel.shape[0]
    halo = -(-(reach - 1) // 16) * 16
    tokens, width = moe_input.shape
    hidden = gate_weight.shape[2]
    cap = 4 * max(1, tokens // n)
    quarter = width // tp
    own_rows = length // tp
    out_width = out_weight.shape[1]
    top = expert_ids.shape[1]
    dma = pltpu.SemaphoreType.DMA
    V = pltpu.VMEM
    pieces = 4
    scratch = dict(
        moe=V((tokens, width), bf16),
        moe_gain=V((1, width), f32),
        ids=V((top, tokens), jnp.int32),
        route=V((top, tokens), f32),
        value=V((length, chan), bf16),
        gate=V((length, chan), bf16),
        taps=V((reach, chan), f32),
        ln_gain=V((1, chan), f32),
        w_gate=V((width, hidden), bf16),
        w_up=V((width, hidden), bf16),
        w_down=V((hidden, width), bf16),
        w_out=V((chan, out_width), bf16),
        load_sem=dma((12,)),
        normed=V((tp, tokens, quarter), bf16),
        ids_all=V((stations, 8, tokens), f32),
        above=V((tokens, tokens), bf16),
        tok=V((stations, 2, tokens, quarter), bf16),
        side=V((stations, 2, cap, quarter), bf16),
        arrived=V((tp, n * cap, quarter), bf16),
        own_send=dma((2, 2)),
        tok_recv=dma((stations, 2)),
        ids_own_send=dma((2,)),
        ids_recv=dma((stations,)),
        pass_send=dma((stations, 2)),
        ids_pass_send=dma((stations,)),
        side_send=dma((stations, 2)),
        side_recv=dma((stations, 2)),
        core_send=dma((n, 2)),
        core_recv=dma((n, 2)),
        cross_send=dma((n,)),
        cross_recv=dma((n,)),
        gated=V((length, chan), bf16),
        halo_in=V((halo, chan), bf16),
        halo_send=dma,
        halo_recv=dma,
        padded=V((length + halo, chan), f32),
        conv=V((length, chan), f32),
        stat_out=V((8, length), f32),
        stat_in=V((tp - 1, 8, length), f32),
        stat_send=dma((tp - 1,)),
        stat_recv=dma((tp - 1,)),
        act=V((length, chan), bf16),
        mix_out=V((2, own_rows, out_width), bf16),
        mix_own=V((2, own_rows, out_width), bf16),
        mix_in=V((2, own_rows, out_width), bf16),
        mix_send=dma((2,)),
        mix_recv=dma((2,)),
        mix_x_out=V((own_rows, out_width), bf16),
        mix_x_in=V((own_rows, out_width), bf16),
        mix_x_send=dma((pieces,)),
        mix_x_recv=dma((pieces,)),
        rs_out=V((n, 2, cap, quarter), bf16),
        rs_own=V((n, 2, cap, quarter), bf16),
        rs_in=V((n, 2, cap, quarter), bf16),
        rs_send=dma((n, 2)),
        rs_recv=dma((n, 2)),
        rx_out=V((n, cap, quarter), bf16),
        rx_in=V((n, cap, quarter), bf16),
        rx_send=dma((n,)),
        rx_recv=dma((n,)),
        answer=V((n, cap, quarter), bf16),
        returned=V((n, cap, quarter), bf16),
        ret_send=dma((n,)),
        ret_recv=dma((n,)),
        total=V((tokens, quarter), f32),
        key=V((tokens, 128), f32),
        weights=V((tokens, 128), f32),
        slant_send=dma((stations,)),
    )
    operands = dict(
        moe_hbm=moe_input,
        moe_gain_hbm=moe_gain.reshape(1, -1),
        ids_hbm=expert_ids.T,
        route_hbm=route_weight.T,
        value_hbm=glu_value,
        gate_hbm=glu_gate,
        taps_hbm=conv_kernel,
        ln_gain_hbm=ln_gain.reshape(1, -1),
        w_gate_hbm=gate_weight,
        w_up_hbm=up_weight,
        w_down_hbm=down_weight,
        w_out_hbm=out_weight,
    )
    names = tuple(operands) + ("mixer_out", "expert_out") + tuple(scratch)
    hbm = pl.BlockSpec(memory_space=pltpu.HBM)
    vmem = pl.BlockSpec(memory_space=pltpu.VMEM)
    mixed, routed = pl.pallas_call(
        functools.partial(line_kernel, n, tp, cap, reach, near, names),
        out_shape=(V((own_rows, out_width), bf16), V((tokens, quarter), bf16)),
        in_specs=[hbm] * len(operands),
        out_specs=(vmem, vmem),
        scratch_shapes=list(scratch.values()),
        compiler_params=pltpu.CompilerParams(
            collective_id=0, has_side_effects=True, vmem_limit_bytes=66_000_000
        ),
        name="line",
    )(*operands.values())
    return settle(
        pltpu.with_memory_space_constraint(mixed, pltpu.VMEM),
        pltpu.with_memory_space_constraint(routed, pltpu.VMEM),
    )


def on_device(
    glu_value,
    glu_gate,
    conv_kernel,
    ln_gain,
    out_weight,
    moe_input,
    moe_gain,
    gate_weight,
    up_weight,
    down_weight,
    expert_ids,
    route_weight,
):
    n = lax.axis_size("ep")
    tp = lax.axis_size("tp")
    chips = tp // 2
    if chips == 2 and (n // 2) * moe_input.shape[0] <= n * 4 * max(1, moe_input.shape[0] // n):
        return line_call(
            3,
            glu_value,
            glu_gate,
            conv_kernel,
            ln_gain,
            out_weight,
            moe_input,
            moe_gain,
            gate_weight,
            up_weight,
            down_weight,
            expert_ids,
            route_weight,
        )
    length, chan = glu_value.shape
    reach = conv_kernel.shape[0]
    halo = -(-(reach - 1) // 16) * 16
    tokens, width = moe_input.shape
    hidden = gate_weight.shape[2]
    cap = 4 * max(1, tokens // n)
    group = max(1, min(n, 256 // cap))
    groups = n // group
    rows = group * cap
    quarter = width // tp
    own_rows = length // tp
    vmem = pl.BlockSpec(memory_space=pltpu.VMEM)
    hbm = pl.BlockSpec(memory_space=pltpu.HBM)
    dma = pltpu.SemaphoreType.DMA
    V = pltpu.VMEM
    others = max(1, chips - 1)
    mixed, routed = pl.pallas_call(
        functools.partial(kernel, n, tp, cap, group, reach),
        out_shape=(
            pltpu.VMEM((own_rows, out_weight.shape[1]), bf16),
            pltpu.VMEM((tokens, quarter), bf16),
        ),
        in_specs=[hbm] * 12,
        out_specs=(vmem, vmem),
        scratch_shapes=[
            V((length, chan), bf16),
            V((length, chan), bf16),
            V(out_weight.shape, bf16),
            V((width, hidden), bf16),
            V((width, hidden), bf16),
            V((hidden, width), bf16),
            dma((6,)),
            V((tokens, width), bf16),
            V((n * cap, quarter), bf16),
            V((chips, cap, quarter), bf16),
            V((n, tokens, cap), bf16),
            V((tp, n * cap, quarter), bf16),
            dma((chips,)),
            dma((chips,)),
            dma((chips,)),
            dma((chips,)),
            dma((n,)),
            dma((n,)),
            dma((n, others)),
            dma((n, others)),
            dma((n,)),
            dma((n,)),
            dma((n, others)),
            dma((n, others)),
            V((length, chan), bf16),
            V((halo, chan), bf16),
            dma,
            dma,
            V((length + halo, chan), f32),
            V((length, chan), f32),
            V((8, length), f32),
            V((tp - 1, 8, length), f32),
            dma((tp - 1,)),
            dma((tp - 1,)),
            V((length, chan), bf16),
            V((chips, own_rows, out_weight.shape[1]), bf16),
            V((chips, own_rows, out_weight.shape[1]), bf16),
            V((chips, own_rows, out_weight.shape[1]), bf16),
            dma((chips,)),
            dma((chips,)),
            V((others, own_rows, out_weight.shape[1]), bf16),
            V((others, own_rows, out_weight.shape[1]), bf16),
            dma((others, 2)),
            dma((others, 2)),
            V((groups, chips, rows, quarter), bf16),
            V((groups, chips, rows, quarter), bf16),
            V((groups, chips, rows, quarter), bf16),
            dma((groups, chips)),
            dma((groups, chips)),
            V((others, n * cap, quarter), bf16),
            V((others, n * cap, quarter), bf16),
            dma((n, others)),
            dma((n, others)),
            V((n * cap, quarter), bf16),
            V((n * cap, quarter), bf16),
            dma((n,)),
            dma((n,)),
            V((tokens, quarter), f32),
            V((tokens, 128), f32),
            V((tokens, width), bf16),
            V((1, width), f32),
            V(expert_ids.T.shape, jnp.int32),
            V(route_weight.T.shape, f32),
            V(conv_kernel.shape, f32),
            V((1, chan), f32),
            dma((6,)),
        ],
        compiler_params=pltpu.CompilerParams(
            collective_id=0, has_side_effects=True, vmem_limit_bytes=66_000_000
        ),
        name="block",
    )(
        moe_input,
        moe_gain.reshape(1, -1),
        expert_ids.T,
        route_weight.T,
        conv_kernel,
        ln_gain.reshape(1, -1),
        glu_value,
        glu_gate,
        out_weight,
        gate_weight,
        up_weight,
        down_weight,
    )
    return settle(
        pltpu.with_memory_space_constraint(mixed, pltpu.VMEM),
        pltpu.with_memory_space_constraint(routed, pltpu.VMEM),
    )


def settle_kernel(a_ref, b_ref, c_ref, d_ref, sem):
    first = pltpu.make_async_copy(a_ref, c_ref, sem.at[0])
    second = pltpu.make_async_copy(b_ref, d_ref, sem.at[1])
    first.start()
    second.start()
    first.wait()
    second.wait()


def settle(a, b):
    vmem = pl.BlockSpec(memory_space=pltpu.VMEM)
    hbm = pl.BlockSpec(memory_space=pltpu.HBM)
    return pl.pallas_call(
        settle_kernel,
        out_shape=(jax.ShapeDtypeStruct(a.shape, a.dtype), jax.ShapeDtypeStruct(b.shape, b.dtype)),
        in_specs=[vmem, vmem],
        out_specs=(hbm, hbm),
        scratch_shapes=[pltpu.SemaphoreType.DMA((2,))],
        name="settle",
    )(a, b)


def solution(mesh):
    in_specs = (
        P("ep", "tp"),
        P("ep", "tp"),
        P(None, "tp"),
        P("tp"),
        P("tp", None),
        P("ep", None),
        P(),
        P("ep", None, "tp"),
        P("ep", None, "tp"),
        P("ep", "tp", None),
        P("ep", None),
        P("ep", None),
    )
    out_specs = (P(("ep", "tp"), None), P("ep", "tp"))
    return jax.shard_map(
        on_device, mesh=mesh, in_specs=in_specs, out_specs=out_specs, check_vma=False
    )
```

```python
import functools
import types

import jax
import jax.numpy as jnp
from jax import lax
from jax.experimental import pallas as pl
from jax.experimental.pallas import tpu as pltpu
from jax.sharding import PartitionSpec as P

eps_rms = 1e-06
eps_norm = 1e-05
MESH = pl.DeviceIdType.MESH
f32 = jnp.float32
bf16 = jnp.bfloat16


def kernel(
    n,
    tp,
    cap,
    group,
    reach,
    moe_hbm,
    moe_gain_hbm,
    ids_t_hbm,
    route_t_hbm,
    taps_hbm,
    ln_gain_hbm,
    value_hbm,
    gate_hbm,
    w_out_hbm,
    w_gate_hbm,
    w_up_hbm,
    w_down_hbm,
    mixer_ref,
    expert_ref,
    value,
    gate,
    w_out,
    w_gate,
    w_up,
    w_down,
    load_sem,
    normed,
    slots,
    near_slots,
    onehots,
    arrived,
    near_send,
    near_recv,
    fn_send,
    fn_recv,
    a2a_send,
    a2a_recv,
    fx_send,
    fx_recv,
    fp_send,
    fp_recv,
    fq_send,
    fq_recv,
    gated,
    halo_in,
    halo_send,
    halo_recv,
    padded,
    conv,
    stat_out,
    stat_in,
    stat_send,
    stat_recv,
    act,
    mix_out,
    mix_own,
    mix_in,
    mix_send,
    mix_recv,
    mix_x_out,
    mix_x_in,
    mix_x_send,
    mix_x_recv,
    rs_out,
    rs_own,
    rs_in,
    rs_send,
    rs_recv,
    rx_out,
    rx_in,
    rx_send,
    rx_recv,
    answer,
    returned,
    ret_send,
    ret_recv,
    total,
    meta_ref,
    moe_ref,
    moe_gain_ref,
    ids_t_ref,
    route_t_ref,
    taps_ref,
    ln_gain_ref,
    small_sem,
):
    me = lax.axis_index("ep")
    mine = lax.axis_index("tp")
    core = lax.rem(mine, 2)
    chip = mine // 2
    partner = chip * 2 + 1 - core
    chips = tp // 2
    groups = n // group
    rows = group * cap
    tokens, width = moe_ref.shape
    quarter = width // tp
    length, chan = value.shape
    halo = halo_in.shape[0]
    own_rows = length // tp

    def toward(k):
        return lax.rem(me // 2 + k // 2, n // 2) * 2 + lax.rem(me + k, 2)

    def source(k):
        return lax.rem(me // 2 + n // 2 - k // 2, n // 2) * 2 + lax.rem(me + k, 2)

    def block(k):
        return pl.ds(pl.multiple_of(k * cap, cap), cap)

    def columns_of(part):
        return pl.ds(pl.multiple_of(part * quarter, 128), quarter)

    def across(j):
        there = lax.rem(chip + j, chips)
        here = lax.rem(chip + chips - j, chips)
        return there * 2 + core, here * 2 + core

    barrier = pltpu.get_barrier_semaphore()

    def greet_ep(k, _):
        pl.semaphore_signal(
            barrier, inc=1, device_id={"ep": lax.rem(me + k, n)}, device_id_type=MESH
        )
        return 0

    lax.fori_loop(1, n, greet_ep, 0)
    for j in range(1, tp):
        pl.semaphore_signal(
            barrier, inc=1, device_id={"tp": lax.rem(mine + j, tp)}, device_id_type=MESH
        )

    loads = [
        pltpu.make_async_copy(src, dst, load_sem.at[i])
        for i, (src, dst) in enumerate(
            [
                (value_hbm, value),
                (gate_hbm, gate),
                (w_out_hbm, w_out),
                (w_gate_hbm.at[0], w_gate),
                (w_up_hbm.at[0], w_up),
                (w_down_hbm.at[0], w_down),
            ]
        )
    ]
    smalls = [
        pltpu.make_async_copy(src, dst, small_sem.at[i])
        for i, (src, dst) in enumerate(
            [
                (moe_hbm, moe_ref),
                (moe_gain_hbm, moe_gain_ref),
                (ids_t_hbm, ids_t_ref),
                (route_t_hbm, route_t_ref),
                (taps_hbm, taps_ref),
                (ln_gain_hbm, ln_gain_ref),
            ]
        )
    ]
    for load in smalls:
        load.start()
    for load in loads:
        load.start()
    for load in smalls:
        load.wait()
    everything = moe_ref[...].astype(f32)
    inverse = lax.rsqrt(jnp.sum(everything * everything, axis=1, keepdims=True) / width + eps_rms)
    normed[...] = (everything * inverse * moe_gain_ref[...]).astype(bf16)
    lead = lax.broadcasted_iota(jnp.int32, (128, tokens), 0)
    meta = jnp.where(lead == 0, ids_t_ref[0:1, :].astype(f32), 0.0)
    meta = jnp.where(lead == 1, ids_t_ref[1:2, :].astype(f32), meta)
    meta = jnp.where(lead == 2, route_t_ref[0:1, :], meta)
    meta = jnp.where(lead == 3, route_t_ref[1:2, :], meta)
    meta_ref[...] = jnp.transpose(meta)
    row = lax.broadcasted_iota(jnp.int32, (tokens, tokens), 0)
    col = lax.broadcasted_iota(jnp.int32, (tokens, tokens), 1)
    below = (col < row).astype(f32).astype(bf16)
    above = (row < col).astype(f32).astype(bf16)

    def a2a_copy(k):
        return pltpu.make_async_remote_copy(
            src_ref=slots.at[block(k)],
            dst_ref=arrived.at[mine, block(k)],
            send_sem=a2a_send.at[k],
            recv_sem=a2a_recv.at[k],
            device_id={"ep": toward(k)},
            device_id_type=MESH,
        )

    def near_copy(xx):
        return pltpu.make_async_remote_copy(
            src_ref=near_slots.at[xx],
            dst_ref=arrived.at[xx * 2 + core, pl.ds(cap, cap)],
            send_sem=near_send.at[xx],
            recv_sem=near_recv.at[xx],
            device_id={"ep": toward(1)},
            device_id_type=MESH,
        )

    def slot_picks(k):
        expert = toward(k)
        member = jnp.maximum(
            (ids_t_ref[0:1, :] == expert).astype(f32), (ids_t_ref[1:2, :] == expert).astype(f32)
        )
        member = jnp.broadcast_to(member, (cap, tokens))
        place = jnp.dot(member.astype(bf16), above, preferred_element_type=f32)
        slot = lax.broadcasted_iota(jnp.int32, (cap, tokens), 0).astype(f32)
        return jnp.where(place == slot, member, 0.0).astype(bf16)

    def picked(pick, part):
        return jnp.dot(
            pick, normed[:, columns_of(part)], preferred_element_type=f32
        ).astype(bf16)

    pl.semaphore_wait(barrier, n - 1 + tp - 1)

    def dispatch(k, _):
        slots[block(k), :] = picked(slot_picks(k), mine)
        a2a_copy(k).start()
        return 0

    loads[0].wait()
    loads[1].wait()
    gated_now = (value[...].astype(f32) * jax.nn.sigmoid(gate[...].astype(f32))).astype(bf16)
    gated[...] = gated_now
    halo_copy = pltpu.make_async_remote_copy(
        src_ref=gated.at[pl.ds(length - halo, halo)],
        dst_ref=halo_in,
        send_sem=halo_send,
        recv_sem=halo_recv,
        device_id={"ep": lax.rem(me + 1, n)},
        device_id_type=MESH,
    )
    halo_copy.start()
    padded[pl.ds(halo, length), :] = gated_now.astype(f32)

    lax.fori_loop(2, n, dispatch, 0)
    pick = slot_picks(1)
    for xx in range(chips):
        near_slots[xx] = picked(pick, xx * 2 + core)
        near_copy(xx).start()

    pick = slot_picks(0)
    for part in range(tp):
        arrived[part, 0:cap, :] = picked(pick, part)

    def fx_copy(k, j):
        to, _ = across(j)
        return pltpu.make_async_remote_copy(
            src_ref=arrived.at[mine, block(k)],
            dst_ref=arrived.at[mine, block(k)],
            send_sem=fx_send.at[k, j - 1],
            recv_sem=fx_recv.at[k, j - 1],
            device_id={"tp": to},
            device_id_type=MESH,
        )

    def fp_copy(k):
        return pltpu.make_async_remote_copy(
            src_ref=arrived.at[mine, block(k)],
            dst_ref=arrived.at[mine, block(k)],
            send_sem=fp_send.at[k],
            recv_sem=fp_recv.at[k],
            device_id={"tp": partner},
            device_id_type=MESH,
        )

    def fq_copy(k, j):
        _, origin = across(j)
        return pltpu.make_async_remote_copy(
            src_ref=arrived.at[origin, block(k)],
            dst_ref=arrived.at[origin, block(k)],
            send_sem=fq_send.at[k, j - 1],
            recv_sem=fq_recv.at[k, j - 1],
            device_id={"tp": partner},
            device_id_type=MESH,
        )

    def fn_copy(xx):
        return pltpu.make_async_remote_copy(
            src_ref=arrived.at[xx * 2 + core, pl.ds(cap, cap)],
            dst_ref=arrived.at[xx * 2 + core, pl.ds(cap, cap)],
            send_sem=fn_send.at[xx],
            recv_sem=fn_recv.at[xx],
            device_id={"tp": partner},
            device_id_type=MESH,
        )

    def over_group(g, do, first=2):
        def one(k, _):
            @pl.when(k >= first)
            def _():
                do(k)

            return 0

        lax.fori_loop(g * group, (g + 1) * group, one, 0)

    def forward_first(g):
        def one(k):
            a2a_copy(k).wait_recv()
            for j in range(1, chips):
                fx_copy(k, j).start()
            fp_copy(k).start()

        over_group(g, one)

    def forward_second(g):
        def one(k):
            for j in range(1, chips):
                fx_copy(k, j).wait_recv()
                fq_copy(k, j).start()

        over_group(g, one)

    def forward_near():
        for xx in range(chips):
            near_copy(xx).wait_recv()
            fn_copy(xx).start()

    halo_copy.wait_recv()
    padded[pl.ds(0, halo), :] = jnp.where(me == 0, 0.0, halo_in[...].astype(f32))
    step_rows = 64
    window = step_rows + halo

    for lane in range(0, chan, 128):

        def conv_step(i, _):
            base = pl.multiple_of(i * step_rows, step_rows)
            rows_in = padded[pl.ds(base, window), lane : lane + 128]
            result = jnp.zeros((step_rows, 128), f32)
            for shift in range(8):
                turned = rows_in if shift == 0 else pltpu.roll(rows_in, window - shift, 0)
                for tap in range(reach):
                    offset = halo - tap
                    if offset % 8 == shift:
                        begin = offset - shift
                        result = (
                            result
                            + taps_ref[tap : tap + 1, lane : lane + 128]
                            * turned[begin : begin + step_rows]
                        )
            conv[pl.ds(base, step_rows), lane : lane + 128] = result
            return 0

        lax.fori_loop(0, length // step_rows, conv_step, 0)

    convolved = conv[...]
    sums = jnp.sum(convolved, axis=1, keepdims=True)
    squares = jnp.sum(convolved * convolved, axis=1, keepdims=True)
    lanes = lax.broadcasted_iota(jnp.int32, (length, 128), 1)
    packed = jnp.where(lanes == 0, sums, jnp.where(lanes == 1, squares, 0.0))
    stat_out[...] = jnp.transpose(packed)[0:8]

    def stat_copy(j):
        return pltpu.make_async_remote_copy(
            src_ref=stat_out,
            dst_ref=stat_in.at[j - 1],
            send_sem=stat_send.at[j - 1],
            recv_sem=stat_recv.at[j - 1],
            device_id={"tp": lax.rem(mine + j, tp)},
            device_id_type=MESH,
        )

    for j in range(1, tp):
        stat_copy(j).start()

    forward_near()
    forward_first(0)
    if groups > 1:
        forward_first(1)
    forward_second(0)

    stats = stat_out[...]
    for j in range(1, tp):
        stat_copy(j).wait_recv()
        stats = stats + stat_in[j - 1]
    stats = jnp.concatenate([stats, jnp.zeros((120, length), f32)], axis=0)
    columns = jnp.transpose(stats)
    mean = columns[:, 0:1] / (chan * tp)
    variance = columns[:, 1:2] / (chan * tp) - mean * mean
    scaled = (conv[...] - mean) * lax.rsqrt(variance + eps_norm) * ln_gain_ref[...]
    act[...] = jax.nn.silu(scaled).astype(bf16)

    def mix_copy(xx):
        return pltpu.make_async_remote_copy(
            src_ref=mix_out.at[xx],
            dst_ref=mix_in.at[xx],
            send_sem=mix_send.at[xx],
            recv_sem=mix_recv.at[xx],
            device_id={"tp": partner},
            device_id_type=MESH,
        )

    def mix_part(owner):
        begin = pl.multiple_of(owner * own_rows, own_rows)
        return jnp.dot(act[pl.ds(begin, own_rows), :], w_out[...], preferred_element_type=f32)

    loads[2].wait()

    def mix_first(xx, _):
        mix_out[xx] = mix_part(xx * 2 + 1 - core).astype(bf16)
        mix_copy(xx).start()
        return 0

    def mix_second(xx, _):
        mix_own[xx] = mix_part(xx * 2 + core).astype(bf16)
        return 0

    lax.fori_loop(0, chips, mix_first, 0)
    lax.fori_loop(0, chips, mix_second, 0)

    half = own_rows // 2

    def mix_x_copy(j, part):
        to, _ = across(j)
        span = pl.ds(part * half, half)
        return pltpu.make_async_remote_copy(
            src_ref=mix_x_out.at[j - 1, span],
            dst_ref=mix_x_in.at[j - 1, span],
            send_sem=mix_x_send.at[j - 1, part],
            recv_sem=mix_x_recv.at[j - 1, part],
            device_id={"tp": to},
            device_id_type=MESH,
        )

    def mix_stage():
        for xx in range(chips):
            mix_copy(xx).wait_recv()
        for j in range(1, chips):
            there = lax.rem(chip + j, chips)
            mix_x_out[j - 1] = (mix_own[there].astype(f32) + mix_in[there].astype(f32)).astype(
                bf16
            )
    loads[3].wait()
    loads[4].wait()
    loads[5].wait()

    def rs_copy(g, xx):
        return pltpu.make_async_remote_copy(
            src_ref=rs_out.at[g, xx],
            dst_ref=rs_in.at[g, xx],
            send_sem=rs_send.at[g, xx],
            recv_sem=rs_recv.at[g, xx],
            device_id={"tp": partner},
            device_id_type=MESH,
        )

    def rx_copy(k, j):
        to, _ = across(j)
        return pltpu.make_async_remote_copy(
            src_ref=rx_out.at[j - 1, block(k)],
            dst_ref=rx_in.at[j - 1, block(k)],
            send_sem=rx_send.at[k, j - 1],
            recv_sem=rx_recv.at[k, j - 1],
            device_id={"tp": to},
            device_id_type=MESH,
        )

    def ret_copy(k):
        return pltpu.make_async_remote_copy(
            src_ref=answer.at[block(k)],
            dst_ref=returned.at[block(k)],
            send_sem=ret_send.at[k],
            recv_sem=ret_recv.at[k],
            device_id={"ep": source(k)},
            device_id_type=MESH,
        )

    def expert_step(g):
        @pl.when(g == 0)
        def _():
            for xx in range(chips):
                fn_copy(xx).wait_recv()

        def one(k):
            fp_copy(k).wait_recv()
            for j in range(1, chips):
                fq_copy(k, j).wait_recv()

        over_group(g, one)
        span = pl.ds(pl.multiple_of(g * rows, rows), rows)
        x = jnp.concatenate([arrived[part, span] for part in range(tp)], axis=1)
        gate_act = jnp.dot(x, w_gate[...], preferred_element_type=f32)
        up_act = jnp.dot(x, w_up[...], preferred_element_type=f32)
        hidden = (jax.nn.silu(gate_act) * up_act).astype(bf16)
        for xx in range(chips):
            begin = pl.multiple_of((xx * 2 + 1 - core) * quarter, 128)
            rs_out[g, xx] = jnp.dot(
                hidden, w_down[:, pl.ds(begin, quarter)], preferred_element_type=f32
            ).astype(bf16)
            rs_copy(g, xx).start()
        for xx in range(chips):
            begin = pl.multiple_of((xx * 2 + core) * quarter, 128)
            rs_own[g, xx] = jnp.dot(
                hidden, w_down[:, pl.ds(begin, quarter)], preferred_element_type=f32
            ).astype(bf16)

    def sum_step(g):
        for xx in range(chips):
            rs_copy(g, xx).wait_recv()
        span = pl.ds(pl.multiple_of(g * rows, rows), rows)
        for j in range(1, chips):
            there = lax.rem(chip + j, chips)
            rx_out[j - 1, span] = (
                rs_own[g, there].astype(f32) + rs_in[g, there].astype(f32)
            ).astype(bf16)

        def one(k):
            for j in range(1, chips):
                rx_copy(k, j).start()

        over_group(g, one, 0)

    def return_step(g):
        def one(k):
            inner = pl.ds(pl.multiple_of((k - g * group) * cap, cap), cap)
            result = rs_own[g, chip, inner].astype(f32) + rs_in[g, chip, inner].astype(f32)
            for j in range(1, chips):
                rx_copy(k, j).wait_recv()
                result = result + rx_in[j - 1, block(k)].astype(f32)
            answer[block(k), :] = result.astype(bf16)

            @pl.when(k > 0)
            def _():
                ret_copy(k).start()

        over_group(g, one, 0)

    total[...] = jnp.zeros_like(total)

    def combine_step(g):
        def take(k, _):
            @pl.when(k > 0)
            def _():
                ret_copy(k).wait_recv()

            expert = toward(k)
            weight = jnp.where(meta_ref[:, 0:1] == expert.astype(f32), meta_ref[:, 2:3], 0.0) + jnp.where(
                meta_ref[:, 1:2] == expert.astype(f32), meta_ref[:, 3:4], 0.0
            )
            answers = returned[block(k), :]
            total[...] += weight * jnp.dot(onehots[k], answers, preferred_element_type=f32)
            return 0

        lax.fori_loop(g * group, (g + 1) * group, take, 0)

    def place_of(k, _):
        expert = toward(k)
        member = jnp.maximum(
            (meta_ref[:, 0:1] == expert.astype(f32)).astype(f32), (meta_ref[:, 1:2] == expert.astype(f32)).astype(f32)
        )
        member = jnp.broadcast_to(member, (tokens, cap))
        place = jnp.dot(below, member.astype(bf16), preferred_element_type=f32)
        slot = lax.broadcasted_iota(jnp.int32, (tokens, cap), 1).astype(f32)
        onehots[k] = jnp.where(place == slot, member, 0.0).astype(bf16)
        return 0

    def step(g, _):
        @pl.when(g < groups)
        def _():
            expert_step(g)

        @pl.when(g < groups)
        def _():
            sum_step(g)

        @pl.when(g + 1 < groups)
        def _():
            forward_second(g + 1)

        @pl.when(g == groups)
        def _():
            lax.fori_loop(0, n, place_of, 0)

        @pl.when((g >= 1) & (g < groups + 1))
        def _():
            return_step(g - 1)

        @pl.when(g == 0)
        def _():
            mix_stage()

        @pl.when(g + 2 < groups)
        def _():
            forward_first(g + 2)

        @pl.when(g == groups - 1)
        def _():
            for j in range(1, chips):
                mix_x_copy(j, 0).start()
                mix_x_copy(j, 1).start()

        return 0

    lax.fori_loop(0, groups + 1, step, 0)
    returned[0:cap, :] = answer[0:cap, :]

    def combine(g, _):
        combine_step(g)
        return 0

    lax.fori_loop(0, groups, combine, 0)
    expert_ref[...] = total[...].astype(bf16)

    mixed = mix_own[chip].astype(f32) + mix_in[chip].astype(f32)
    for j in range(1, chips):
        mix_x_copy(j, 0).wait_recv()
        mix_x_copy(j, 1).wait_recv()
        mixed = mixed + mix_x_in[j - 1].astype(f32)
    mixer_ref[...] = mixed.astype(bf16)

    ret_copy(1).wait_send()

    def left(k, _):
        a2a_copy(k).wait_send()
        ret_copy(k).wait_send()
        fp_copy(k).wait_send()
        for j in range(1, chips):
            fx_copy(k, j).wait_send()
            fq_copy(k, j).wait_send()
        return 0

    lax.fori_loop(2, n, left, 0)

    def left_x(k, _):
        for j in range(1, chips):
            rx_copy(k, j).wait_send()
        return 0

    lax.fori_loop(0, n, left_x, 0)
    halo_copy.wait_send()
    for j in range(1, tp):
        stat_copy(j).wait_send()
    for xx in range(chips):
        mix_copy(xx).wait_send()
        near_copy(xx).wait_send()
        fn_copy(xx).wait_send()
    for j in range(1, chips):
        mix_x_copy(j, 0).wait_send()
        mix_x_copy(j, 1).wait_send()

    def left_group(g, _):
        for xx in range(chips):
            rs_copy(g, xx).wait_send()
        return 0

    lax.fori_loop(0, groups, left_group, 0)


def line_kernel(n, tp, cap, reach, near, names, *refs):
    r = types.SimpleNamespace(**dict(zip(names, refs)))
    me = lax.axis_index("ep")
    mine = lax.axis_index("tp")
    core = lax.rem(mine, 2)
    chip = mine // 2
    partner = chip * 2 + 1 - core
    across = (1 - chip) * 2 + core
    stations = n // 2
    z = me // 2
    y = lax.rem(me, 2)
    beside = z * 2 + 1 - y
    tokens, width = r.moe.shape
    quarter = width // tp
    length, chan = r.value.shape
    halo = r.halo_in.shape[0]
    own_rows = length // tp
    behind = jnp.minimum(z, stations - 1 - z)
    inner = behind >= 1
    longer = jnp.where(stations - 1 - z > z, 1, -1)

    reach_here = jnp.where(inner, near[1], near[0])

    def distance(j):
        return jnp.where(j <= 2 * behind, (j + 1) // 2, j - behind)

    def origin(j):
        turn = jnp.where((j <= 2 * behind) & (lax.rem(j, 2) == 1), -longer, longer)
        return z + turn * distance(j)

    def home(s):
        return origin(s // 2) * 2 + lax.rem(y + s, 2)

    def block(k):
        return pl.ds(pl.multiple_of(k * cap, cap), cap)

    def remote(src, dst, send, recv, **device):
        return pltpu.make_async_remote_copy(
            src_ref=src,
            dst_ref=dst,
            send_sem=send,
            recv_sem=recv,
            device_id=device,
            device_id_type=MESH,
        )

    barrier = pltpu.get_barrier_semaphore()

    def greet_ep(k, _):
        pl.semaphore_signal(
            barrier, inc=1, device_id={"ep": lax.rem(me + k, n)}, device_id_type=MESH
        )
        return 0

    lax.fori_loop(1, n, greet_ep, 0)
    for j in range(1, tp):
        pl.semaphore_signal(
            barrier, inc=1, device_id={"tp": lax.rem(mine + j, tp)}, device_id_type=MESH
        )

    loads = {
        name: pltpu.make_async_copy(src, dst, r.load_sem.at[i])
        for i, (name, src, dst) in enumerate(
            [
                ("moe", r.moe_hbm.at[pl.ds(0, tokens // 2)], r.moe.at[pl.ds(0, tokens // 2)]),
                ("more", r.moe_hbm.at[pl.ds(tokens // 2, tokens // 2)], r.moe.at[pl.ds(tokens // 2, tokens // 2)]),
                ("moe_gain", r.moe_gain_hbm, r.moe_gain),
                ("ids", r.ids_hbm, r.ids),
                ("route", r.route_hbm, r.route),
                ("value", r.value_hbm, r.value),
                ("gate", r.gate_hbm, r.gate),
                ("taps", r.taps_hbm, r.taps),
                ("ln_gain", r.ln_gain_hbm, r.ln_gain),
                ("w_gate", r.w_gate_hbm.at[0], r.w_gate),
                ("w_up", r.w_up_hbm.at[0], r.w_up),
                ("w_down", r.w_down_hbm.at[0], r.w_down),
                ("w_out", r.w_out_hbm, r.w_out),
            ]
        )
    }
    late = ("w_gate", "w_up", "w_down", "w_out")
    for name, load in loads.items():
        if name not in late:
            load.start()

    def own_copy(up):
        return remote(
            r.normed.at[mine],
            r.tok.at[z, chip],
            r.own_send.at[up],
            r.tok_recv.at[z, chip],
            ep=(z + 2 * up - 1) * 2 + y,
        )

    half = tokens // 2

    def rest_copy(zz, up, part):
        span = pl.ds(part * half, half)
        return remote(
            r.normed.at[across, span],
            r.tok.at[zz, 1 - chip, span],
            r.rest_send.at[up, part],
            r.rest_recv.at[zz, part],
            ep=(z + 2 * up - 1) * 2 + y,
        )

    def passes_rest(j):
        there = onward(origin(j))
        wanted = jnp.where((there == 0) | (there == stations - 1), near[0], near[1])
        return (there >= 0) & (there < stations) & (distance(j) + 1 < wanted)

    def own_ids(up):
        return remote(
            r.ids_all.at[z],
            r.ids_all.at[z],
            r.ids_own_send.at[up],
            r.ids_recv.at[z],
            ep=(z + 2 * up - 1) * 2 + y,
        )

    def onward(zz):
        return jnp.where(zz < z, z + 1, z - 1)

    def pass_copy(zz, xx):
        return remote(
            r.tok.at[zz, xx],
            r.tok.at[zz, xx],
            r.pass_send.at[zz, xx],
            r.tok_recv.at[zz, xx],
            ep=onward(zz) * 2 + y,
        )

    def pass_ids(zz):
        return remote(
            r.ids_all.at[zz],
            r.ids_all.at[zz],
            r.ids_pass_send.at[zz],
            r.ids_recv.at[zz],
            ep=onward(zz) * 2 + y,
        )

    def side_copy(j, xx):
        return remote(
            r.side.at[j, xx],
            r.arrived.at[xx * 2 + core, block(2 * j + 1)],
            r.side_send.at[j, xx],
            r.side_recv.at[j, xx],
            ep=beside,
        )

    def slant_copy(j):
        return remote(
            r.side.at[j, chip],
            r.arrived.at[mine, block(2 * j + 1)],
            r.slant_send.at[j],
            r.side_recv.at[j, chip],
            ep=beside,
            tp=across,
        )

    def core_copy(s, xx):
        return remote(
            r.arrived.at[xx * 2 + core, block(s)],
            r.arrived.at[xx * 2 + core, block(s)],
            r.core_send.at[s, xx],
            r.core_recv.at[s, xx],
            tp=partner,
        )

    def cross_copy(s):
        return remote(
            r.arrived.at[mine, block(s)],
            r.arrived.at[mine, block(s)],
            r.cross_send.at[s],
            r.cross_recv.at[s],
            tp=across,
        )

    def rs_copy(s, xx):
        return remote(
            r.rs_out.at[s, xx], r.rs_in.at[s, xx], r.rs_send.at[s, xx], r.rs_recv.at[s, xx], tp=partner
        )

    def rx_copy(s):
        return remote(r.rx_out.at[s], r.rx_in.at[s], r.rx_send.at[s], r.rx_recv.at[s], tp=across)

    def ret_copy(s):
        return remote(
            r.answer.at[s], r.returned.at[me], r.ret_send.at[s], r.ret_recv.at[me], ep=home(s)
        )

    def ret_arrival(s):
        there = home(s)
        return remote(
            r.answer.at[s], r.returned.at[there], r.ret_send.at[s], r.ret_recv.at[there], ep=there
        )

    halo_copy = remote(
        r.gated.at[pl.ds(length - halo, halo)],
        r.halo_in,
        r.halo_send,
        r.halo_recv,
        ep=lax.rem(me + 1, n),
    )

    def stat_copy(j):
        return remote(
            r.stat_out,
            r.stat_in.at[j - 1],
            r.stat_send.at[j - 1],
            r.stat_recv.at[j - 1],
            tp=lax.rem(mine + j, tp),
        )

    def mix_copy(xx):
        return remote(r.mix_out.at[xx], r.mix_in.at[xx], r.mix_send.at[xx], r.mix_recv.at[xx], tp=partner)

    pieces = r.mix_x_send.shape[0]
    piece = own_rows // pieces

    def mix_x_copy(part):
        span = pl.ds(pl.multiple_of(part * piece, piece), piece)
        return remote(
            r.mix_x_out.at[span], r.mix_x_in.at[span], r.mix_x_send.at[part], r.mix_x_recv.at[part], tp=across
        )

    loads["moe_gain"].wait()
    for name, begin in (("moe", 0), ("more", tokens // 2)):
        loads[name].wait()
        span = pl.ds(begin, tokens // 2)
        everything = r.moe[span].astype(f32)
        inverse = lax.rsqrt(jnp.sum(everything * everything, axis=1, keepdims=True) / width + eps_rms)
        normed_now = (everything * inverse * r.moe_gain[...]).astype(bf16)
        for part in range(tp):
            r.normed[part, span] = normed_now[:, part * quarter : (part + 1) * quarter]
    loads["ids"].wait()
    loads["route"].wait()
    r.ids_all[z] = jnp.concatenate([r.ids[...].astype(f32), jnp.zeros((6, tokens), f32)], axis=0)
    for name in late:
        loads[name].start()
    loads["value"].wait()
    loads["gate"].wait()
    gated_now = (r.value[...].astype(f32) * jax.nn.sigmoid(r.gate[...].astype(f32))).astype(bf16)
    r.gated[...] = gated_now
    r.padded[pl.ds(halo, length), :] = gated_now.astype(f32)

    pl.semaphore_wait(barrier, n - 1 + tp - 1)
    halo_copy.start()

    def each_way(do):
        @pl.when(z > 0)
        def _():
            do(0)

        @pl.when(z < stations - 1)
        def _():
            do(1)

    each_way(lambda up: own_ids(up).start())
    each_way(lambda up: own_copy(up).start())
    each_way(lambda up: rest_copy(z, up, 0).start())

    @pl.when(jnp.logical_not(inner))
    def _():
        each_way(lambda up: rest_copy(z, up, 1).start())

    row = lax.broadcasted_iota(jnp.int32, (tokens, tokens), 0)
    col = lax.broadcasted_iota(jnp.int32, (tokens, tokens), 1)
    r.above[...] = (row < col).astype(f32).astype(bf16)
    slot_rows = lax.broadcasted_iota(jnp.int32, (cap, tokens), 0).astype(f32)

    def choices(zz):
        here = (z * 2 + lax.rem(y + lax.broadcasted_iota(jnp.int32, (16, tokens), 0), 2)).astype(f32)
        chosen = r.ids_all[zz]
        member = jnp.maximum(
            (chosen[0:1, :] == here).astype(f32), (chosen[1:2, :] == here).astype(f32)
        )
        place = jnp.dot(member.astype(bf16), r.above[...], preferred_element_type=f32)
        key = jnp.where(member > 0.0, place, -1.0)
        ours = (slot_rows == key[0:1, :]).astype(f32).astype(bf16)
        theirs = (slot_rows == key[1:2, :]).astype(f32).astype(bf16)
        return ours, theirs

    ours, theirs = choices(z)
    for xx in (chip, 1 - chip):
        r.side[0, xx] = jnp.dot(
            theirs, r.normed[xx * 2 + core], preferred_element_type=f32
        ).astype(bf16)
        side_copy(0, xx).start()
    for part in range(tp):
        r.arrived[part, block(0), :] = jnp.dot(
            ours, r.normed[part], preferred_element_type=f32
        ).astype(bf16)

    def expert_step(s, first=False):
        def partial(part):
            rows = pl.ds(pl.multiple_of(part * quarter, quarter), quarter)
            x = r.arrived[part, block(s)]
            return (
                jnp.dot(x, r.w_gate[rows, :], preferred_element_type=f32),
                jnp.dot(x, r.w_up[rows, :], preferred_element_type=f32),
            )

        gate_act, up_act = partial(core)
        more = partial(2 + core)
        gate_act, up_act = gate_act + more[0], up_act + more[1]
        for xx in range(2):
            if not first:
                core_copy(s, xx).wait_recv()
            more = partial(xx * 2 + 1 - core)
            gate_act, up_act = gate_act + more[0], up_act + more[1]
        hidden = (jax.nn.silu(gate_act) * up_act).astype(bf16)
        for xx in (1 - chip, chip):
            begin = pl.multiple_of((xx * 2 + 1 - core) * quarter, 128)
            r.rs_out[s, xx] = jnp.dot(
                hidden, r.w_down[:, pl.ds(begin, quarter)], preferred_element_type=f32
            ).astype(bf16)
            rs_copy(s, xx).start()
        for xx in (1 - chip, chip):
            begin = pl.multiple_of((xx * 2 + core) * quarter, 128)
            r.rs_own[s, xx] = jnp.dot(
                hidden, r.w_down[:, pl.ds(begin, quarter)], preferred_element_type=f32
            ).astype(bf16)

    def sum_step(s):
        rs_copy(s, 1 - chip).wait_recv()
        r.rx_out[s] = (r.rs_own[s, 1 - chip].astype(f32) + r.rs_in[s, 1 - chip].astype(f32)).astype(bf16)
        rx_copy(s).start()

    def return_step(s):
        rs_copy(s, chip).wait_recv()
        rx_copy(s).wait_recv()
        result = r.rs_own[s, chip].astype(f32) + r.rs_in[s, chip].astype(f32)
        r.answer[s] = (result + r.rx_in[s].astype(f32)).astype(bf16)

        @pl.when(s > 0)
        def _():
            ret_copy(s).start()

    loads["taps"].wait()
    step_rows = 64
    window = step_rows + halo

    def conv_rows(lane, begin, end):
        def conv_step(i, _):
            base = pl.multiple_of(i * step_rows, step_rows)
            rows_in = r.padded[pl.ds(base, window), lane : lane + 128]
            result = jnp.zeros((step_rows, 128), f32)
            for shift in range(8):
                turned = rows_in if shift == 0 else pltpu.roll(rows_in, window - shift, 0)
                for tap in range(reach):
                    offset = halo - tap
                    if offset % 8 == shift:
                        begin = offset - shift
                        result = (
                            result
                            + r.taps[tap : tap + 1, lane : lane + 128]
                            * turned[begin : begin + step_rows]
                        )
            r.conv[pl.ds(base, step_rows), lane : lane + 128] = result
            return 0

        lax.fori_loop(begin, end, conv_step, 0)

    for lane in range(0, chan, 128):
        conv_rows(lane, 1, length // step_rows)
    lead = lax.broadcasted_iota(jnp.int32, (128, tokens), 0)
    meta = jnp.where(lead == 0, r.ids[0:1, :].astype(f32), 0.0)
    meta = jnp.where(lead == 1, r.ids[1:2, :].astype(f32), meta)
    meta = jnp.where(lead == 2, r.route[0:1, :], meta)
    meta = jnp.where(lead == 3, r.route[1:2, :], meta)
    meta = jnp.transpose(meta)
    order = lax.broadcasted_iota(jnp.int32, (tokens, 128), 1)
    expert = home(order).astype(f32)
    first = (meta[:, 0:1] == expert) & (order < n)
    second = (meta[:, 1:2] == expert) & (order < n)
    member = jnp.maximum(first.astype(f32), second.astype(f32))
    below = (col < row).astype(f32).astype(bf16)
    place = jnp.dot(below, member.astype(bf16), preferred_element_type=f32)
    key = jnp.where(member > 0.0, place, -1.0)
    weights = jnp.where(first, meta[:, 2:3], 0.0) + jnp.where(second, meta[:, 3:4], 0.0)
    r.key[...] = key
    r.weights[...] = weights
    halo_copy.wait_recv()
    r.padded[pl.ds(0, halo), :] = jnp.where(me == 0, 0.0, r.halo_in[...].astype(f32))
    for lane in range(0, chan, 128):
        conv_rows(lane, 0, 1)

    convolved = r.conv[...]
    sums = jnp.sum(convolved, axis=1, keepdims=True)
    squares = jnp.sum(convolved * convolved, axis=1, keepdims=True)
    lanes = lax.broadcasted_iota(jnp.int32, (length, 128), 1)
    packed = jnp.where(lanes == 0, sums, jnp.where(lanes == 1, squares, 0.0))
    r.stat_out[...] = jnp.transpose(packed)[0:8]
    for j in range(1, tp):
        stat_copy(j).start()

    loads["w_gate"].wait()
    loads["w_up"].wait()
    loads["w_down"].wait()
    expert_step(0, first=True)

    def pull(j):
        zz = origin(j)
        there = onward(zz)
        pass_ids(zz).wait_recv()
        pass_copy(zz, chip).wait_recv()

        @pl.when((there >= 0) & (there < stations))
        def _():
            pass_ids(zz).start()
            pass_copy(zz, chip).start()

    def pull_rest(j):
        zz = origin(j)
        there = onward(zz)

        @pl.when(distance(j) == 1)
        def _():
            for part in range(2):
                rest_copy(zz, 0, part).wait_recv()

        @pl.when(distance(j) > 1)
        def _():
            pass_copy(zz, 1 - chip).wait_recv()

        @pl.when(passes_rest(j))
        def _():
            pass_copy(zz, 1 - chip).start()

    def spread(j, xx, once):
        zz = origin(j)
        rows = jnp.dot(r.picks[j], r.tok[zz, xx], preferred_element_type=f32).astype(bf16)
        r.side[j, xx] = rows[cap:]
        r.arrived[xx * 2 + core, block(2 * j), :] = rows[:cap]
        side_copy(j, xx).start()
        if once:

            @pl.when(distance(j) >= reach_here)
            def _():
                slant_copy(j).start()
                cross_copy(2 * j).start()

        core_copy(2 * j, xx).start()

    def absorb(j):
        r.picks[j] = jnp.concatenate(choices(origin(j)), axis=0)
        spread(j, chip, True)

    def absorb_rest(j):
        pull_rest(j)
        spread(j, 1 - chip, False)

    def gather_side(j):
        for xx in (chip, 1 - chip):
            side_copy(j, xx).wait_recv()
            core_copy(2 * j + 1, xx).start()

    def gather_cross(s):
        @pl.when((distance(s // 2) >= reach_here) & (lax.rem(s, 2) == 0))
        def _():
            cross_copy(s).wait_recv()
            core_copy(s, 1 - chip).start()

    loads["ln_gain"].wait()
    loads["w_out"].wait()
    sum_step(0)
    stats = r.stat_out[...]
    for j in range(1, tp):
        stat_copy(j).wait_recv()
        stats = stats + r.stat_in[j - 1]
    stats = jnp.concatenate([stats, jnp.zeros((120, length), f32)], axis=0)
    columns = jnp.transpose(stats)
    mean = columns[:, 0:1] / (chan * tp)
    variance = columns[:, 1:2] / (chan * tp) - mean * mean
    scaled = (r.conv[...] - mean) * lax.rsqrt(variance + eps_norm) * r.ln_gain[...]
    r.act[...] = jax.nn.silu(scaled).astype(bf16)

    @pl.when(inner)
    def _():
        pull(1)
        pull(2)
        each_way(lambda up: rest_copy(z, up, 1).start())

    def mix_part(owner):
        begin = pl.multiple_of(owner * own_rows, own_rows)
        return jnp.dot(r.act[pl.ds(begin, own_rows), :], r.w_out[...], preferred_element_type=f32)

    for xx in (1 - chip, chip):
        r.mix_out[xx] = mix_part(xx * 2 + 1 - core).astype(bf16)
        mix_copy(xx).start()
        r.mix_own[xx] = mix_part(xx * 2 + core).astype(bf16)
    mix_copy(1 - chip).wait_recv()
    for part in range(pieces):
        span = pl.ds(part * piece, piece)
        r.mix_x_out[span] = (
            r.mix_own[1 - chip, span].astype(f32) + r.mix_in[1 - chip, span].astype(f32)
        ).astype(bf16)
    mix_x_copy(0).start()

    plan = schedule(stations)
    early = min(pieces - 1, 2)

    def entry(name, i):
        found = jnp.int32(-1)
        for k, (end, mid) in enumerate(plan[name]):
            found = jnp.where(i == k, jnp.where(inner, mid, end), found)
        return found

    def step(i, _):
        a = entry("arrive", i)
        e = entry("expert", i)
        b = entry("answer", i)
        c = entry("pull", i)
        d = entry("sum", i)
        g = entry("rest", i)
        h = entry("before", i)
        j = a // 2

        @pl.when(c >= 0)
        def _():
            pull(c)

        @pl.when((a >= 0) & (lax.rem(a, 2) == 0))
        def _():
            @pl.when(jnp.logical_not(inner))
            def _():
                pull(j)

            absorb(j)

        @pl.when((a >= 0) & (lax.rem(a, 2) == 1))
        def _():
            gather_side(j)

        @pl.when((g >= 0) & (distance(g // 2) < reach_here))
        def _():
            absorb_rest(g // 2)

        @pl.when(h >= 0)
        def _():
            sum_step(h)

        @pl.when(e >= 0)
        def _():
            gather_cross(e)
            expert_step(e)

        @pl.when(b >= 0)
        def _():
            return_step(b)

        @pl.when(d >= 0)
        def _():
            sum_step(d)

        @pl.when((i + 1 <= early) & jnp.logical_not(inner))
        def _():
            mix_x_copy(i + 1).start()

        return 0

    lax.fori_loop(0, len(plan["arrive"]), step, 0)

    slot_columns = lax.broadcasted_iota(jnp.int32, (tokens, cap), 1).astype(f32)

    def take(s):
        onehot = (r.key[:, s : s + 1] == slot_columns).astype(f32).astype(bf16)
        if s > 0:
            ret_arrival(s).wait_recv()
            rows = r.returned[home(s)]
        else:
            rows = r.answer[0]
        return r.weights[:, s : s + 1] * jnp.dot(onehot, rows, preferred_element_type=f32)

    for part in range(1, pieces):
        if part > early:
            mix_x_copy(part).start()
        else:

            @pl.when(inner)
            def _():
                mix_x_copy(part).start()

    for k in range(len(plan["finish"])):
        b = jnp.where(inner, *reversed(plan["finish"][k]))

        @pl.when(b >= 0)
        def _():
            return_step(b)

        if k == 0:
            r.total[...] = take(0)
        elif k == 1:
            r.total[...] += take(1)

    rest = [s for s in range(2, n) if s % 2 == 0] + [s for s in range(n - 1, 2, -2)]
    for s in rest[:-2]:
        r.total[...] += take(s)
    mix_copy(chip).wait_recv()
    mixed = r.mix_own[chip].astype(f32) + r.mix_in[chip].astype(f32)
    for part in range(pieces):
        mix_x_copy(part).wait_recv()
    r.mixer_out[...] = (mixed + r.mix_x_in[...].astype(f32)).astype(bf16)
    for s in rest[-2:-1]:
        r.total[...] += take(s)
    r.expert_out[...] = (r.total[...] + take(rest[-1])).astype(bf16)

    each_way(lambda up: own_ids(up).wait_send())
    each_way(lambda up: own_copy(up).wait_send())
    each_way(lambda up: rest_copy(z, up, 0).wait_send())
    each_way(lambda up: rest_copy(z, up, 1).wait_send())

    def left(j, _):
        zz = origin(j)
        there = onward(zz)
        full = distance(j) < reach_here

        @pl.when((there >= 0) & (there < stations))
        def _():
            pass_ids(zz).wait_send()
            pass_copy(zz, chip).wait_send()

        @pl.when(passes_rest(j))
        def _():
            pass_copy(zz, 1 - chip).wait_send()

        side_copy(j, chip).wait_send()

        @pl.when(full)
        def _():
            side_copy(j, 1 - chip).wait_send()

        for s in (2 * j, 2 * j + 1):
            for xx in range(2):
                core_copy(s, xx).wait_send()

        @pl.when(jnp.logical_not(full))
        def _():
            cross_copy(2 * j).wait_send()
            slant_copy(j).wait_send()

        return 0

    lax.fori_loop(1, stations, left, 0)
    for xx in range(2):
        side_copy(0, xx).wait_send()
        core_copy(1, xx).wait_send()
        mix_copy(xx).wait_send()

    def left_more(s, _):
        for xx in range(2):
            rs_copy(s, xx).wait_send()
        rx_copy(s).wait_send()

        @pl.when(s > 0)
        def _():
            ret_copy(s).wait_send()

        return 0

    lax.fori_loop(0, n, left_more, 0)
    halo_copy.wait_send()
    for j in range(1, tp):
        stat_copy(j).wait_send()
    for part in range(pieces):
        mix_x_copy(part).wait_send()


def schedule(stations):
    total = 2 * stations
    if stations == 4:
        ends = dict(
            arrive=[1, 2, 4, -1, 6, 3, -1, 7, 5],
            rest=[-1, -1, -1, 2, -1, -1, 4],
            expert=[1, -1, -1, 2, -1, 3, 4, 7, 6, 5],
            sum=[1, -1, -1, 2, -1, 3, 4, 7, 6, 5],
            answer=[-1, 0, -1, -1, -1, 1, -1, 2, 3, 4],
            finish=[7, 6, 5],
        )
        mids = dict(
            arrive=[4, 1, 2, 6, 3, 7, 5],
            rest=[-1, -1, 2, 4],
            expert=[-1, 1, 2, 4, 3, 7, 6, 5],
            sum=[-1, 1, -1, 2, 4, 7, 6, 5, 3],
            pull=[-1, -1, -1, 3],
            answer=[-1, -1, 0, -1, -1, 1, 4, -1, 7],
            finish=[6, 5, 2, 3],
        )
    else:
        arrive = [1] + list(range(2, total, 2)) + list(range(3, total, 2))
        count = len(arrive)
        ends = dict(
            arrive=arrive,
            rest=[-1] + list(range(2, total, 2)),
            expert=[1] + [-1] * (count - 1) + list(range(2, total)),
            finish=list(range(total)),
        )
        ends["sum"] = ends["expert"]
        mids = dict(ends, pull=[-1] + list(range(3, stations)))
    plan = {}
    steps = max(len(part) for part in list(ends.values()) + list(mids.values()))
    for name in ("arrive", "rest", "before", "expert", "sum", "answer", "pull", "finish"):
        one, two = ends.get(name, []), mids.get(name, [])
        used = max(len(one), len(two)) if name == "finish" else steps
        plan[name] = [tuple((part + [-1] * used)[k] for part in (one, two)) for k in range(used)]
    return plan


def line_call(
    near,
    glu_value,
    glu_gate,
    conv_kernel,
    ln_gain,
    out_weight,
    moe_input,
    moe_gain,
    gate_weight,
    up_weight,
    down_weight,
    expert_ids,
    route_weight,
):
    n = lax.axis_size("ep")
    tp = lax.axis_size("tp")
    stations = n // 2
    length, chan = glu_value.shape
    reach = conv_kernel.shape[0]
    halo = -(-(reach - 1) // 16) * 16
    tokens, width = moe_input.shape
    hidden = gate_weight.shape[2]
    cap = 4 * max(1, tokens // n)
    quarter = width // tp
    own_rows = length // tp
    out_width = out_weight.shape[1]
    top = expert_ids.shape[1]
    dma = pltpu.SemaphoreType.DMA
    V = pltpu.VMEM
    pieces = 4
    scratch = dict(
        moe=V((tokens, width), bf16),
        moe_gain=V((1, width), f32),
        ids=V((top, tokens), jnp.int32),
        route=V((top, tokens), f32),
        value=V((length, chan), bf16),
        gate=V((length, chan), bf16),
        taps=V((reach, chan), f32),
        ln_gain=V((1, chan), f32),
        w_gate=V((width, hidden), bf16),
        w_up=V((width, hidden), bf16),
        w_down=V((hidden, width), bf16),
        w_out=V((chan, out_width), bf16),
        load_sem=dma((13,)),
        normed=V((tp, tokens, quarter), bf16),
        ids_all=V((stations, 8, tokens), f32),
        above=V((tokens, tokens), bf16),
        tok=V((stations, 2, tokens, quarter), bf16),
        side=V((stations, 2, cap, quarter), bf16),
        arrived=V((tp, n * cap, quarter), bf16),
        own_send=dma((2,)),
        rest_send=dma((2, 2)),
        rest_recv=dma((stations, 2)),
        picks=V((stations, 2 * cap, tokens), bf16),
        tok_recv=dma((stations, 2)),
        ids_own_send=dma((2,)),
        ids_recv=dma((stations,)),
        pass_send=dma((stations, 2)),
        ids_pass_send=dma((stations,)),
        side_send=dma((stations, 2)),
        side_recv=dma((stations, 2)),
        core_send=dma((n, 2)),
        core_recv=dma((n, 2)),
        cross_send=dma((n,)),
        cross_recv=dma((n,)),
        gated=V((length, chan), bf16),
        halo_in=V((halo, chan), bf16),
        halo_send=dma,
        halo_recv=dma,
        padded=V((length + halo, chan), f32),
        conv=V((length, chan), f32),
        stat_out=V((8, length), f32),
        stat_in=V((tp - 1, 8, length), f32),
        stat_send=dma((tp - 1,)),
        stat_recv=dma((tp - 1,)),
        act=V((length, chan), bf16),
        mix_out=V((2, own_rows, out_width), bf16),
        mix_own=V((2, own_rows, out_width), bf16),
        mix_in=V((2, own_rows, out_width), bf16),
        mix_send=dma((2,)),
        mix_recv=dma((2,)),
        mix_x_out=V((own_rows, out_width), bf16),
        mix_x_in=V((own_rows, out_width), bf16),
        mix_x_send=dma((pieces,)),
        mix_x_recv=dma((pieces,)),
        rs_out=V((n, 2, cap, quarter), bf16),
        rs_own=V((n, 2, cap, quarter), bf16),
        rs_in=V((n, 2, cap, quarter), bf16),
        rs_send=dma((n, 2)),
        rs_recv=dma((n, 2)),
        rx_out=V((n, cap, quarter), bf16),
        rx_in=V((n, cap, quarter), bf16),
        rx_send=dma((n,)),
        rx_recv=dma((n,)),
        answer=V((n, cap, quarter), bf16),
        returned=V((n, cap, quarter), bf16),
        ret_send=dma((n,)),
        ret_recv=dma((n,)),
        total=V((tokens, quarter), f32),
        key=V((tokens, 128), f32),
        weights=V((tokens, 128), f32),
        slant_send=dma((stations,)),
    )
    operands = dict(
        moe_hbm=moe_input,
        moe_gain_hbm=moe_gain.reshape(1, -1),
        ids_hbm=expert_ids.T,
        route_hbm=route_weight.T,
        value_hbm=glu_value,
        gate_hbm=glu_gate,
        taps_hbm=conv_kernel,
        ln_gain_hbm=ln_gain.reshape(1, -1),
        w_gate_hbm=gate_weight,
        w_up_hbm=up_weight,
        w_down_hbm=down_weight,
        w_out_hbm=out_weight,
    )
    names = tuple(operands) + ("mixer_out", "expert_out") + tuple(scratch)
    hbm = pl.BlockSpec(memory_space=pltpu.HBM)
    vmem = pl.BlockSpec(memory_space=pltpu.VMEM)
    mixed, routed = pl.pallas_call(
        functools.partial(line_kernel, n, tp, cap, reach, near, names),
        out_shape=(V((own_rows, out_width), bf16), V((tokens, quarter), bf16)),
        in_specs=[hbm] * len(operands),
        out_specs=(vmem, vmem),
        scratch_shapes=list(scratch.values()),
        compiler_params=pltpu.CompilerParams(
            collective_id=0, has_side_effects=True, vmem_limit_bytes=66_000_000
        ),
        name="line",
    )(*operands.values())
    return settle(
        pltpu.with_memory_space_constraint(mixed, pltpu.VMEM),
        pltpu.with_memory_space_constraint(routed, pltpu.VMEM),
    )


def on_device(
    glu_value,
    glu_gate,
    conv_kernel,
    ln_gain,
    out_weight,
    moe_input,
    moe_gain,
    gate_weight,
    up_weight,
    down_weight,
    expert_ids,
    route_weight,
):
    n = lax.axis_size("ep")
    tp = lax.axis_size("tp")
    chips = tp // 2
    if chips == 2 and (n // 2) * moe_input.shape[0] <= n * 4 * max(1, moe_input.shape[0] // n):
        return line_call(
            (3, 2),
            glu_value,
            glu_gate,
            conv_kernel,
            ln_gain,
            out_weight,
            moe_input,
            moe_gain,
            gate_weight,
            up_weight,
            down_weight,
            expert_ids,
            route_weight,
        )
    length, chan = glu_value.shape
    reach = conv_kernel.shape[0]
    halo = -(-(reach - 1) // 16) * 16
    tokens, width = moe_input.shape
    hidden = gate_weight.shape[2]
    cap = 4 * max(1, tokens // n)
    group = max(1, min(n, 256 // cap))
    groups = n // group
    rows = group * cap
    quarter = width // tp
    own_rows = length // tp
    vmem = pl.BlockSpec(memory_space=pltpu.VMEM)
    hbm = pl.BlockSpec(memory_space=pltpu.HBM)
    dma = pltpu.SemaphoreType.DMA
    V = pltpu.VMEM
    others = max(1, chips - 1)
    mixed, routed = pl.pallas_call(
        functools.partial(kernel, n, tp, cap, group, reach),
        out_shape=(
            pltpu.VMEM((own_rows, out_weight.shape[1]), bf16),
            pltpu.VMEM((tokens, quarter), bf16),
        ),
        in_specs=[hbm] * 12,
        out_specs=(vmem, vmem),
        scratch_shapes=[
            V((length, chan), bf16),
            V((length, chan), bf16),
            V(out_weight.shape, bf16),
            V((width, hidden), bf16),
            V((width, hidden), bf16),
            V((hidden, width), bf16),
            dma((6,)),
            V((tokens, width), bf16),
            V((n * cap, quarter), bf16),
            V((chips, cap, quarter), bf16),
            V((n, tokens, cap), bf16),
            V((tp, n * cap, quarter), bf16),
            dma((chips,)),
            dma((chips,)),
            dma((chips,)),
            dma((chips,)),
            dma((n,)),
            dma((n,)),
            dma((n, others)),
            dma((n, others)),
            dma((n,)),
            dma((n,)),
            dma((n, others)),
            dma((n, others)),
            V((length, chan), bf16),
            V((halo, chan), bf16),
            dma,
            dma,
            V((length + halo, chan), f32),
            V((length, chan), f32),
            V((8, length), f32),
            V((tp - 1, 8, length), f32),
            dma((tp - 1,)),
            dma((tp - 1,)),
            V((length, chan), bf16),
            V((chips, own_rows, out_weight.shape[1]), bf16),
            V((chips, own_rows, out_weight.shape[1]), bf16),
            V((chips, own_rows, out_weight.shape[1]), bf16),
            dma((chips,)),
            dma((chips,)),
            V((others, own_rows, out_weight.shape[1]), bf16),
            V((others, own_rows, out_weight.shape[1]), bf16),
            dma((others, 2)),
            dma((others, 2)),
            V((groups, chips, rows, quarter), bf16),
            V((groups, chips, rows, quarter), bf16),
            V((groups, chips, rows, quarter), bf16),
            dma((groups, chips)),
            dma((groups, chips)),
            V((others, n * cap, quarter), bf16),
            V((others, n * cap, quarter), bf16),
            dma((n, others)),
            dma((n, others)),
            V((n * cap, quarter), bf16),
            V((n * cap, quarter), bf16),
            dma((n,)),
            dma((n,)),
            V((tokens, quarter), f32),
            V((tokens, 128), f32),
            V((tokens, width), bf16),
            V((1, width), f32),
            V(expert_ids.T.shape, jnp.int32),
            V(route_weight.T.shape, f32),
            V(conv_kernel.shape, f32),
            V((1, chan), f32),
            dma((6,)),
        ],
        compiler_params=pltpu.CompilerParams(
            collective_id=0, has_side_effects=True, vmem_limit_bytes=66_000_000
        ),
        name="block",
    )(
        moe_input,
        moe_gain.reshape(1, -1),
        expert_ids.T,
        route_weight.T,
        conv_kernel,
        ln_gain.reshape(1, -1),
        glu_value,
        glu_gate,
        out_weight,
        gate_weight,
        up_weight,
        down_weight,
    )
    return settle(
        pltpu.with_memory_space_constraint(mixed, pltpu.VMEM),
        pltpu.with_memory_space_constraint(routed, pltpu.VMEM),
    )


def settle_kernel(a_ref, b_ref, c_ref, d_ref, sem):
    first = pltpu.make_async_copy(a_ref, c_ref, sem.at[0])
    second = pltpu.make_async_copy(b_ref, d_ref, sem.at[1])
    first.start()
    second.start()
    first.wait()
    second.wait()


def settle(a, b):
    vmem = pl.BlockSpec(memory_space=pltpu.VMEM)
    hbm = pl.BlockSpec(memory_space=pltpu.HBM)
    return pl.pallas_call(
        settle_kernel,
        out_shape=(jax.ShapeDtypeStruct(a.shape, a.dtype), jax.ShapeDtypeStruct(b.shape, b.dtype)),
        in_specs=[vmem, vmem],
        out_specs=(hbm, hbm),
        scratch_shapes=[pltpu.SemaphoreType.DMA((2,))],
        name="settle",
    )(a, b)


def solution(mesh):
    in_specs = (
        P("ep", "tp"),
        P("ep", "tp"),
        P(None, "tp"),
        P("tp"),
        P("tp", None),
        P("ep", None),
        P(),
        P("ep", None, "tp"),
        P("ep", None, "tp"),
        P("ep", "tp", None),
        P("ep", None),
        P("ep", None),
    )
    out_specs = (P(("ep", "tp"), None), P("ep", "tp"))
    return jax.shard_map(
        on_device, mesh=mesh, in_specs=in_specs, out_specs=out_specs, check_vma=False
    )
```
